128 devices in a mesh: sp: 16 (over z, y), dp: 8 (over x, core).
Axes of the slice: x: 4, y: 4, z: 4, core: 2. Of those that a mesh axis runs over, the one named last changes fastest.
Arguments:
- residual_input: bfloat16 [8, 2048, 2048], P('dp', 'sp'), may hold values from -6 to 6
- queries: bfloat16 [8, 2048, 1024], P('dp', 'sp'), may hold values from -6 to 6
- keys: bfloat16 [8, 2048, 1024], P('dp', 'sp'), may hold values from -6 to 6
- values: bfloat16 [8, 2048, 2048], P('dp', 'sp'), may hold values from -6 to 6
- gate_logits: bfloat16 [8, 2048, 64], P('dp', 'sp'), may hold values from -6 to 6
- retention_offset: float32 [16, 2], P('sp'), may hold values from 3 to 12
- log_forget_extra: float32 [8, 16, 2048], P('dp', 'sp'), may hold values from -2.76 to 0
- lane_amplifier: float32 [2048], P('sp'), may hold values from 0.1 to 1.9
- output_gate_logits: bfloat16 [8, 2048, 2048], P('dp', 'sp'), may hold values from -6 to 6
- output_projection: bfloat16 [2048, 2048], P(None, 'dp'), may hold values from -0.125 to 0.125
- cell_norm_gain: float32 [2048], replicated, may hold values from 0.1 to 1.9
- expert_norm_gain: float32 [2048], replicated, may hold values from 0.1 to 1.9
- expert_index: int32 [8, 2048, 2], P('dp', 'sp'), may hold values from 0 to 127, all different within a row; in each aligned block of 128 rows (0 to 127, 128 to 255, ..., all dimensions but the last counted through in order) at most 4 rows name the same one
- group_mixing_weight: float32 [8, 2048, 4], P('dp', 'sp'), may hold values from 0.05 to 1
- within_group_weight: float32 [8, 2048, 2], P('dp', 'sp'), may hold values from 0.1 to 1
- gate_weight: bfloat16 [128, 2048, 1024], P(('sp', 'dp')), may hold values from -0.125 to 0.125
- up_weight: bfloat16 [128, 2048, 1024], P(('sp', 'dp')), may hold values from -0.125 to 0.125
- down_weight: bfloat16 [128, 1024, 2048], P(('sp', 'dp')), may hold values from -0.75 to 0.75
Outputs:
- stream_out: bfloat16 [8, 2048, 2048], P('dp', 'sp')
The draws below stay inside these ranges and needn't reach their ends.
Inputs may be any that keep to these rules, and one draw needn't show every extreme that they name: `expert_index`: A token's two experts differ; among the 128 tokens of one device no expert is named more than 4 times, a bound that some block reaches.
All inputs are finite; a program needn't handle non-finite values.
Results may differ from the reference program's by a relative error of at most 0.0095.
Values may be sent and summed in bfloat16 or wider, within the bound.
A program may use at most 128 MiB of HBM per device.

```python
import math
from functools import partial
import jax
import jax.numpy as jnp
import numpy as np
from jax import lax

D = 2048
DK = 64
CONTENT_WIDTH = 128
ATTENTION_LANES = 16
W_A = 2048
FF = 1024
GROUPS = 4
EXPERTS = 128
SPAN_STEPS = 512
T_DEV = 128
SEQS = 8
LEN = 2048
TOKENS = 16384
CAP = 4


def draw_log_forget_extra(key, part):
    first_key, second_key = jax.random.split(jax.random.fold_in(key, 17))
    places = jax.random.randint(first_key, (SEQS, ATTENTION_LANES, 4), 0, LEN)
    depth = jax.random.uniform(second_key, (SEQS, ATTENTION_LANES, 4), jnp.float32, 0.22, 0.69)
    positions = jnp.arange(LEN, dtype=jnp.int32)
    struck = places[:, :, :, None] == positions[None, None, None, :]
    return -jnp.sum(jnp.where(struck, depth[:, :, :, None], 0.0), axis=2).astype(jnp.float32)


def steps_of(own_key, extent, shards, smallest, largest):
    factor_of, own = 1.0, jax.random.fold_in(own_key, 6)
    for position, parts in shards:
        heights = jnp.exp(jax.random.uniform(jax.random.fold_in(own, position), (parts,), jnp.float32, smallest / len(shards), largest / len(shards)))
        factor_of = factor_of * jnp.repeat(heights, extent[position] // parts).reshape([-1 if axis == position else 1 for axis in range(len(extent))])
    return factor_of


def assign_block(key, own, number, rows, number_of, top, limit, skew):
    order = jax.random.permutation(key, number_of)
    heavy_load, ordinary = shares(number_of, rows * top, limit, skew, True), shares(number_of, rows * top, limit, skew, False)
    places = jnp.arange(number_of)

    def named(sizes, offset_by):
        used = int((sizes > 0).sum())
        fixed = max(1, used // 4)
        passed = fixed + (places - fixed + offset_by * (used - fixed)) % max(1, number_of - fixed)
        return jnp.zeros((number_of,), jnp.int32).at[order[jnp.where(places < fixed, places, passed)]].set(jnp.asarray(sizes, jnp.int32))

    sizes = jnp.where(number % 4 == 0, named(heavy_load, number // 4), named(ordinary, number - number // 4 - 1))
    mixed = jax.random.permutation(jax.random.fold_in(own, 3), number_of)
    donor, sink = mixed[0:number_of // 2 * 2:2], mixed[1:number_of // 2 * 2:2]
    slack = jnp.minimum(sizes[donor] - 1, limit - sizes[sink]) // 2
    slack = jnp.where((donor == order[0]) | (sink == order[0]) | (sizes[sink] == 0), 0, jnp.maximum(slack, 0))
    passed = jax.random.randint(jax.random.fold_in(own, 4), (number_of // 2,), 0, 1 << 20) % (slack + 1)
    sizes = sizes.at[donor].add(-passed).at[sink].add(passed)
    items = jnp.searchsorted(jnp.cumsum(sizes), jnp.arange(rows * top), side="right").astype(jnp.int32)
    listing = items.reshape(top, rows).T
    listing = listing[jax.random.permutation(jax.random.fold_in(own, 1), rows)]
    offset_by = jax.random.randint(jax.random.fold_in(own, 2), (rows, 1), 0, top)
    return jnp.take_along_axis(listing, (jnp.arange(top)[None, :] + offset_by) % top, axis=1)


def shares(count, total, bound, lean, full):
    loads = [(1 << 20) // math.isqrt(standing ** lean) + 1 for standing in range(1, count + 1)]
    largest = bound if full else min(bound, max(-(-total // count), total * loads[0] // sum(loads)))
    least = 1 if total - largest >= count - 1 else 0
    counts, spare = [largest] + [least] * (count - 1), total - largest - least * (count - 1)
    while spare > 0:
        movable = [i for i in range(1, count) if counts[i] < largest] or [i for i in range(1, count) if counts[i] < bound]
        pool, remaining = sum([loads[i] for i in movable]), spare
        for i in movable:
            extra = min(bound - counts[i], max(1, remaining * loads[i] // pool), spare)
            counts[i] = counts[i] + extra
            spare = spare - extra
    return np.array(counts)


def normal_values(own_key, extent, deviation, most, shards=(), held_as=jnp.bfloat16):
    factor_of = steps_of(own_key, extent, shards, -0.22, 0.18) if shards else 1.0
    result = jax.random.normal(own_key, extent, jnp.float32) * deviation * factor_of
    return jnp.minimum(jnp.maximum(result, -most), most).astype(held_as)


def setup_inputs(seed: int = 0) -> dict:
    arg_keys = jax.random.split(jax.random.key(seed), 19)
    residual_input = normal_values(arg_keys[0], (SEQS, LEN, D), 1.0, 6.0, ((0, 8), (1, 16)))
    queries = normal_values(arg_keys[1], (SEQS, LEN, ATTENTION_LANES * DK), 1.0, 6.0, ((0, 8), (1, 16)))
    keys = normal_values(arg_keys[2], (SEQS, LEN, ATTENTION_LANES * DK), 1.0, 6.0, ((0, 8), (1, 16)))
    values = normal_values(arg_keys[3], (SEQS, LEN, W_A), 1.0, 6.0, ((0, 8), (1, 16)))
    gate_logits = normal_values(arg_keys[4], (SEQS, LEN, 4 * ATTENTION_LANES), 1.0, 6.0, ((0, 8), (1, 16)))
    retention_offset = jnp.clip(3.0 + 9.0 * jax.random.uniform(arg_keys[5], (ATTENTION_LANES, 2), jnp.float32) ** steps_of(arg_keys[5], (ATTENTION_LANES, 2), ((0, 16),), -0.2, 0.2), 3.0, 12.0)
    log_forget_extra = draw_log_forget_extra(jax.random.fold_in(arg_keys[18], 71), 0)
    lane_amplifier = jnp.clip(1.0 + 0.18 * jax.random.normal(arg_keys[7], (W_A,), jnp.float32), 0.1, 1.9)
    output_gate_logits = normal_values(arg_keys[8], (SEQS, LEN, W_A), 1.0, 6.0, ((0, 8), (1, 16)))
    output_projection = normal_values(arg_keys[9], (W_A, D), W_A ** -0.5, 0.125, ((1, 8),))
    cell_norm_gain = jnp.clip(1.0 + 0.18 * jax.random.normal(arg_keys[10], (D,), jnp.float32), 0.1, 1.9)
    expert_norm_gain = jnp.clip(1.0 + 0.18 * jax.random.normal(arg_keys[11], (D,), jnp.float32), 0.1, 1.9)
    expert_index_keys = jax.random.split(jax.random.fold_in(arg_keys[12], 1), SEQS * LEN // T_DEV)
    expert_index_turns = jax.random.permutation(jax.random.fold_in(arg_keys[12], 3), SEQS * LEN // T_DEV)
    expert_index = jax.vmap(lambda own, number: assign_block(jax.random.fold_in(arg_keys[12], 2), own, number, T_DEV, EXPERTS, 2, CAP, 2))(expert_index_keys, expert_index_turns).reshape((SEQS, LEN, 2))
    group_mixing_weight = jnp.clip(0.05 + 0.95 * jax.random.uniform(arg_keys[13], (SEQS, LEN, GROUPS), jnp.float32) ** steps_of(arg_keys[13], (SEQS, LEN, GROUPS), ((0, 8), (1, 16)), -0.2, 0.2), 0.05, 1.0)
    within_group_weight = jnp.clip(0.1 + 0.9 * jax.random.uniform(arg_keys[14], (SEQS, LEN, 2), jnp.float32) ** steps_of(arg_keys[14], (SEQS, LEN, 2), ((0, 8), (1, 16)), -0.2, 0.2), 0.1, 1.0)
    gate_weight = normal_values(arg_keys[15], (EXPERTS, D, FF), D ** -0.5, 0.125, ((0, 128),))
    up_weight = normal_values(arg_keys[16], (EXPERTS, D, FF), D ** -0.5, 0.125, ((0, 128),))
    down_weight = normal_values(arg_keys[17], (EXPERTS, FF, D), (FF // 16) ** -0.5, 0.75, ((0, 128),))
    return dict(residual_input=residual_input, queries=queries, keys=keys, values=values, gate_logits=gate_logits, retention_offset=retention_offset, log_forget_extra=log_forget_extra, lane_amplifier=lane_amplifier, output_gate_logits=output_gate_logits, output_projection=output_projection, cell_norm_gain=cell_norm_gain, expert_norm_gain=expert_norm_gain, expert_index=expert_index, group_mixing_weight=group_mixing_weight, within_group_weight=within_group_weight, gate_weight=gate_weight, up_weight=up_weight, down_weight=down_weight)


EPS = 1e-06
HIGH_PRECISION = lax.Precision.HIGHEST

def block_states(keys_f, values_f, in_gate, log_forget, span_steps):
    length, key_width = keys_f.shape
    blocks = length // span_steps
    blocked_keys = keys_f.reshape(blocks, span_steps, key_width)
    blocked_values = values_f.reshape(blocks, span_steps, values_f.shape[1])
    running = jnp.cumsum(log_forget.reshape(blocks, span_steps), axis=1)
    block_end = running[:, -1]
    weight_log = block_end[:, None] - running + in_gate.reshape(blocks, span_steps)
    local_top = lax.optimization_barrier(jnp.max(weight_log, axis=1))
    weight_table = jnp.exp(weight_log - local_top[:, None])
    local_memory = jnp.einsum('ryd,rya->rda', blocked_values * weight_table[:, :, None], blocked_keys, precision=HIGH_PRECISION)
    local_normalizer = jnp.einsum('nb,nby->ny', weight_table, blocked_keys, precision=HIGH_PRECISION)

    def advance(carried_state, inputs):
        memory, normal, stable = carried_state
        end_log, top_log, memory_new, normal_new = inputs
        raised = jnp.maximum(end_log + stable, top_log)
        keep_old = jnp.exp(end_log + stable - raised)
        keep_new = jnp.exp(top_log - raised)
        updated = (keep_old * memory + keep_new * memory_new, keep_old * normal + keep_new * normal_new, raised)
        return (updated, (memory, normal, stable))
    initial = (jnp.zeros((values_f.shape[1], key_width), jnp.float32), jnp.zeros((key_width,), jnp.float32), jnp.zeros((), jnp.float32))
    _, entries = lax.scan(advance, initial, (block_end, local_top, local_memory, local_normalizer))
    return entries

def direction_out(query_f, keys_f, values_f, in_gate, log_forget, span_steps):
    entry_memory, entry_normal, entry_top = block_states(keys_f, values_f, in_gate, log_forget, span_steps)
    length, key_width = keys_f.shape
    blocks = length // span_steps
    query_blocks = query_f.reshape(blocks, span_steps, key_width) * key_width ** (-0.5)
    blocked_keys = keys_f.reshape(blocks, span_steps, key_width)
    blocked_values = values_f.reshape(blocks, span_steps, values_f.shape[1])
    running = jnp.cumsum(log_forget.reshape(blocks, span_steps), axis=1)
    entry_log = running + entry_top[:, None]
    pair_log = running[:, :, None] - running[:, None, :] + in_gate.reshape(blocks, span_steps)[:, None, :]
    earlier = jnp.tril(jnp.ones((span_steps, span_steps), dtype=bool))
    pair_log = jnp.where(earlier[None], pair_log, -jnp.inf)
    top_log = jnp.maximum(entry_log, lax.optimization_barrier(jnp.max(pair_log, axis=2)))
    scores = jnp.einsum('ctk,csk->cts', query_blocks, blocked_keys, precision=HIGH_PRECISION) * jnp.exp(pair_log - top_log[:, :, None])
    carried = jnp.exp(entry_log - top_log)
    numerator = carried[:, :, None] * jnp.einsum('cvk,ctk->ctv', entry_memory, query_blocks, precision=HIGH_PRECISION)
    numerator = numerator + jnp.einsum('cts,csv->ctv', scores, blocked_values, precision=HIGH_PRECISION)
    denominator = carried * jnp.einsum('ck,ctk->ct', entry_normal, query_blocks, precision=HIGH_PRECISION) + lax.optimization_barrier(jnp.sum(scores, axis=2))
    output = numerator / jnp.maximum(jnp.abs(denominator), jnp.exp(-top_log))[:, :, None]
    return output.reshape(length, blocked_values.shape[2])

def lane_blend(lane_question, lane_addresses, lane_contents, lane_switches, lane_offset, lane_spread, lane_rescaling, span_steps):
    query_f = lane_question.astype(jnp.float32)
    keys_f = lane_addresses.astype(jnp.float32)
    values_f = lane_contents.astype(jnp.float32)
    retention_entries = lane_switches.astype(jnp.float32)
    onward_fading = jax.nn.log_sigmoid(retention_entries[:, 1] + lane_offset[0]) + lane_spread
    reverse_fading = jax.nn.log_sigmoid(retention_entries[:, 3] + lane_offset[1]) + lane_spread
    forward = direction_out(query_f, keys_f, values_f, retention_entries[:, 0], onward_fading, span_steps)
    backward = direction_out(query_f[::-1], keys_f[::-1], values_f[::-1], retention_entries[::-1, 2], reverse_fading[::-1], span_steps)[::-1]
    total = forward + backward
    normed = total * lax.rsqrt(lax.optimization_barrier(jnp.mean(total * total, axis=1, keepdims=True)) + EPS) * lane_rescaling
    return normed.astype(jnp.bfloat16)

def series_blender(series_question, series_addresses, series_contents, series_switches, series_spread, retention_offset, lane_amplifier):
    lane_question = series_question.reshape(LEN, ATTENTION_LANES, DK).transpose(1, 0, 2)
    lane_addresses = series_addresses.reshape(LEN, ATTENTION_LANES, DK).transpose(1, 0, 2)
    lane_contents = series_contents.reshape(LEN, ATTENTION_LANES, CONTENT_WIDTH).transpose(1, 0, 2)
    lane_switches = series_switches.reshape(LEN, ATTENTION_LANES, 4).transpose(1, 0, 2)
    return jax.vmap(partial(lane_blend, span_steps=SPAN_STEPS))(lane_question, lane_addresses, lane_contents, lane_switches, retention_offset, series_spread, lane_amplifier.reshape(ATTENTION_LANES, CONTENT_WIDTH))

def reference(residual_input, queries, keys, values, gate_logits, retention_offset, log_forget_extra, lane_amplifier, output_gate_logits, output_projection, cell_norm_gain, expert_norm_gain, expert_index, group_mixing_weight, within_group_weight, gate_weight, up_weight, down_weight):
    mixed_output = lax.map(lambda packed_rows: series_blender(packed_rows[0], packed_rows[1], packed_rows[2], packed_rows[3], packed_rows[4], retention_offset, lane_amplifier), (queries, keys, values, gate_logits, log_forget_extra))
    mixed_output = mixed_output.transpose(0, 2, 1, 3).reshape(TOKENS, W_A)
    gated = (mixed_output.astype(jnp.float32) * jax.nn.sigmoid(output_gate_logits.reshape(TOKENS, W_A).astype(jnp.float32))).astype(jnp.bfloat16)
    proj = jnp.dot(gated, output_projection, preferred_element_type=jnp.float32)
    stream_f = residual_input.reshape(TOKENS, D).astype(jnp.float32)
    stream = (stream_f + cell_norm_gain * proj * lax.rsqrt(lax.optimization_barrier(jnp.mean(proj * proj, axis=1, keepdims=True)) + EPS)).astype(jnp.bfloat16)
    stream_f = stream.astype(jnp.float32)
    moe_in = (expert_norm_gain * stream_f * lax.rsqrt(lax.optimization_barrier(jnp.mean(stream_f * stream_f, axis=1, keepdims=True)) + EPS)).astype(jnp.bfloat16)
    dev_blocks = TOKENS // T_DEV
    flat_ids = expert_index.reshape(TOKENS * 2)
    block_ids = flat_ids.reshape(dev_blocks, T_DEV * 2)
    onehot = (block_ids[:, :, None] == jnp.arange(EXPERTS, dtype=jnp.int32)[None, None, :]).astype(jnp.int32)
    slot_index = lax.optimization_barrier(jnp.sum((jnp.cumsum(onehot, axis=1) - onehot) * onehot, axis=2))
    column = (jnp.arange(dev_blocks, dtype=jnp.int32)[:, None] * CAP + slot_index).reshape(TOKENS * 2).astype(jnp.int32)
    token_of = (jnp.arange(TOKENS * 2, dtype=jnp.int32) // 2).astype(jnp.int32)
    group_of = expert_index.reshape(TOKENS, 2) // (EXPERTS // GROUPS)
    group_hit = (group_of[:, :, None] == jnp.arange(GROUPS, dtype=jnp.int32)[None, None, :]).astype(jnp.float32)
    chosen_group = lax.optimization_barrier(jnp.sum(group_mixing_weight.reshape(TOKENS, 1, GROUPS) * group_hit, axis=2))
    route = (chosen_group * within_group_weight.reshape(TOKENS, 2)).reshape(TOKENS * 2)
    table = jnp.full((EXPERTS, dev_blocks * CAP), TOKENS, jnp.int32).at[flat_ids, column].set(token_of)
    share = jnp.zeros((EXPERTS, dev_blocks * CAP), jnp.float32).at[flat_ids, column].set(route)
    padded = jnp.concatenate([moe_in, jnp.zeros((1, D), jnp.bfloat16)], axis=0)

    def expert_pass(total, inputs):
        rows_index, rows_share, gate_w, up_w, down_w = inputs
        picked = padded[rows_index]
        hidden = (jax.nn.silu(jnp.dot(picked, gate_w, preferred_element_type=jnp.float32)) * jnp.dot(picked, up_w, preferred_element_type=jnp.float32)).astype(jnp.bfloat16)
        produced = jnp.dot(hidden, down_w, preferred_element_type=jnp.float32).astype(jnp.bfloat16)
        return (total.at[rows_index].add(rows_share[:, None] * produced.astype(jnp.float32)), None)
    total, _ = lax.scan(expert_pass, jnp.zeros((TOKENS + 1, D), jnp.float32), (table, share, gate_weight, up_weight, down_weight))
    stream_out = (stream_f + total[:TOKENS]).astype(jnp.bfloat16)
    return stream_out.reshape(SEQS, LEN, D)
```

```python
from functools import partial

import jax
import jax.numpy as jnp
from jax import lax
from jax.experimental import pallas as pl
from jax.experimental.pallas import tpu as pltpu
from jax.sharding import PartitionSpec as P

EPS = 1e-06
HIGH = lax.Precision.HIGHEST
F32 = jnp.float32
BF16 = jnp.bfloat16
H = 16
DK = 64
DV = 128
C = 128
PAIRS = H // 2
NT = (((1,), (1,)), ((), ()))
TN = (((0,), (0,)), ((), ()))


def log_sigmoid(x):
    return jnp.minimum(x, 0.0) - jnp.log1p(jnp.exp(-jnp.abs(x)))


def cell_kernel(
    q_ref, k_ref, v_ref, g_ref, msg_ref, ogl_ref,
    out_ref,
    rx1, lst, lsm, rxs, rxm, ent, enm, est, esm,
    fcol, bcol, rows, nfb, zfb, sg,
    sa, ra, sb, rb, sc, rc, sd, rd, se, re,
):
    me = lax.axis_index("sp")

    def peer_of(d):
        return lax.rem(me + d, H)

    def remote(src, dst, ssem, rsem, peer):
        return pltpu.make_async_remote_copy(
            src_ref=src, dst_ref=dst, send_sem=ssem, recv_sem=rsem,
            device_id={"sp": peer}, device_id_type=pl.DeviceIdType.MESH,
        )

    def each_peer(body):
        def step(d, carry):
            body(peer_of(d))
            return carry

        lax.fori_loop(1, H, step, 0)

    barrier = pltpu.get_barrier_semaphore()
    each_peer(lambda p: pl.semaphore_signal(
        barrier, inc=1, device_id={"sp": p}, device_id_type=pl.DeviceIdType.MESH))
    pl.semaphore_wait(barrier, H - 1)

    each_peer(lambda p: remote(msg_ref.at[p], rx1.at[me], sa.at[p], ra.at[me], p).start())
    rx1[me] = msg_ref[me]

    lane = lax.broadcasted_iota(jnp.int32, (C, C), 1)
    low_half = lane < DK
    row_id = lax.broadcasted_iota(jnp.int32, (C, C), 0)
    earlier = lane <= row_id
    diagonal = lane == row_id

    def gate_step(p, carry):
        cols = pl.ds(pl.multiple_of(p * 256, 256), 256)
        sg[:, cols] = 1.0 / (1.0 + jnp.exp(-ogl_ref[:, cols].astype(F32)))
        return carry

    lax.fori_loop(0, PAIRS, gate_step, 0)

    each_peer(lambda p: remote(msg_ref.at[p], rx1.at[p], sa.at[p], ra.at[p], p).wait_recv())

    spread = rx1[:, 0, :]
    in_f = g_ref[0]
    in_b = g_ref[2]
    fade_f = log_sigmoid(g_ref[1] + rx1[:, 2, :]) + spread
    fade_b = log_sigmoid(g_ref[3] + rx1[:, 3, :]) + spread
    upto = (row_id <= lane).astype(F32)
    since = (row_id >= lane).astype(F32)
    cum_f = lax.dot_general(fade_f, upto, (((1,), (0,)), ((), ())), precision=HIGH, preferred_element_type=F32)
    cum_b = lax.dot_general(fade_b, since, (((1,), (0,)), ((), ())), precision=HIGH, preferred_element_type=F32)
    end_f = jnp.broadcast_to(cum_f[:, C - 1:C], (H, C))
    end_b = jnp.broadcast_to(cum_b[:, 0:1], (H, C))
    w_f = jnp.exp(end_f - cum_f + in_f)
    w_b = jnp.exp(end_b - cum_b + in_b)
    rows[0] = cum_f - in_f
    rows[1] = cum_b - in_b
    rows[2] = jnp.exp(in_b)
    turned = jnp.concatenate([cum_f, cum_b, w_f, w_b, jnp.zeros((C - 4 * H, C), F32)], axis=0).T
    wf_hi = w_f.astype(BF16)
    wb_hi = w_b.astype(BF16)
    wf_lo = (w_f - wf_hi.astype(F32)).astype(BF16)
    wb_lo = (w_b - wb_hi.astype(F32)).astype(BF16)
    stacked = jnp.concatenate([wf_hi, wf_lo, wb_hi, wb_lo], axis=0)
    for p in range(PAIRS):
        cols = slice(p * C, (p + 1) * C)
        kp = k_ref[:, cols]
        k32 = kp.astype(F32)
        h0, h1 = 2 * p, 2 * p + 1
        wf = jnp.where(low_half, turned[:, 32 + h0:33 + h0], turned[:, 32 + h1:33 + h1])
        wb = jnp.where(low_half, turned[:, 48 + h0:49 + h0], turned[:, 48 + h1:49 + h1])
        both = jnp.concatenate([k32 * wf, k32 * wb], axis=1).astype(BF16)
        state = lax.dot_general(both, v_ref[:, p * 256:(p + 1) * 256], TN, preferred_element_type=F32).astype(BF16)
        lst[h0, 0] = state[0:64, 0:128]
        lst[h1, 0] = state[64:128, 128:256]
        lst[h0, 1] = state[128:192, 0:128]
        lst[h1, 1] = state[192:256, 128:256]
        norm = jnp.dot(stacked, kp, preferred_element_type=F32)
        norm_f = norm[0:16] + norm[16:32]
        norm_b = norm[32:48] + norm[48:64]
        low_row = low_half[0:1]
        for hh, h in ((0, h0), (1, h1)):
            keep = low_row if hh == 0 else ~low_row
            nf = norm_f[h:h + 1]
            nb = norm_b[h:h + 1]
            nf = jnp.where(keep, nf, pltpu.roll(nf, DK, 1))
            nb = jnp.where(keep, nb, pltpu.roll(nb, DK, 1))
            lsm[h] = jnp.concatenate(
                [nf, nb, end_f[h:h + 1], end_b[h:h + 1], jnp.zeros((4, C), F32)], axis=0)

    each_peer(lambda p: remote(lsm.at[p], rxm.at[me], sc.at[p], rc.at[me], p).start())
    each_peer(lambda p: remote(lst.at[p], rxs.at[me], sb.at[p], rb.at[me], p).start())
    rxs[me] = lst[me]
    rxm[me] = lsm[me]

    for h in range(H):
        fcol[h] = jnp.broadcast_to(turned[:, h:h + 1], (C, C))
        bcol[h] = jnp.broadcast_to(turned[:, 16 + h:17 + h], (C, C))

    def lhs_of(cols):
        qp = q_ref[:, cols] * jnp.asarray(DK ** -0.5, BF16)
        none = jnp.zeros_like(qp)
        return jnp.concatenate([jnp.where(low_half, qp, none), jnp.where(low_half, none, qp)], axis=0)

    def inner_step(p, carry):
        cols = pl.ds(pl.multiple_of(p * C, C), C)
        score2 = lax.dot_general(lhs_of(cols), k_ref[:, cols], NT, preferred_element_type=F32)
        for hh in range(2):
            h = 2 * p + hh
            score = score2[hh * C:(hh + 1) * C]
            ahead = fcol[h] - rows[0, pl.ds(h, 1), :]
            behind = bcol[h] - rows[1, pl.ds(h, 1), :]
            weighted = score * jnp.exp(jnp.where(earlier, ahead, behind))
            pf = jnp.where(earlier, weighted, 0.0)
            pb = jnp.where(earlier, jnp.where(diagonal, score * rows[2, pl.ds(h, 1), :], 0.0), weighted)
            both = jnp.concatenate([pf, pb], axis=0)
            zfb[h] = jnp.broadcast_to(jnp.sum(both, axis=1, keepdims=True), (2 * C, C))
            vcols = pl.ds(pl.multiple_of(h * DV, DV), DV)
            nfb[h] = jnp.dot(both.astype(BF16), v_ref[:, vcols], preferred_element_type=F32)
        return carry

    lax.fori_loop(0, PAIRS, inner_step, 0)

    each_peer(lambda p: remote(lsm.at[p], rxm.at[p], sc.at[p], rc.at[p], p).wait_recv())
    each_peer(lambda p: remote(lst.at[p], rxs.at[p], sb.at[p], rb.at[p], p).wait_recv())

    def carry_step(c, state):
        mf, mb, nf, nb = state
        d = H - 1 - c
        ent[c, 0] = mf.astype(BF16)
        ent[d, 1] = mb.astype(BF16)
        enm[c, 0:1] = nf
        enm[d, 1:2] = nb
        keep_f = jnp.exp(rxm[c, 2:3])
        keep_b = jnp.exp(rxm[d, 3:4])
        return (
            mf * keep_f + rxs[c, 0].astype(F32),
            mb * keep_b + rxs[d, 1].astype(F32),
            nf * keep_f + rxm[c, 0:1],
            nb * keep_b + rxm[d, 1:2],
        )

    zero_m = jnp.zeros((DK, DV), F32)
    zero_n = jnp.zeros((1, C), F32)
    enm[...] = jnp.zeros_like(enm)
    lax.fori_loop(0, H, carry_step, (zero_m, zero_m, zero_n, zero_n))

    def slot(h):
        return est.at[lax.div(h, 2), :, pl.ds(pl.multiple_of(lax.rem(h, 2) * DK, DK), DK), :]

    each_peer(lambda p: remote(enm.at[p], esm.at[me], sd.at[p], rd.at[me], p).start())
    each_peer(lambda p: remote(ent.at[p], slot(me), se.at[p], re.at[me], p).start())
    esm[me] = enm[me]
    est[lax.div(me, 2), :, pl.ds(pl.multiple_of(lax.rem(me, 2) * DK, DK), DK), :] = ent[me]

    def outer_step(p, carry):
        for hh in range(2):
            h = 2 * p + hh

            @pl.when(h != me)
            def _():
                remote(enm.at[h], esm.at[h], sd.at[h], rd.at[h], h).wait_recv()
                remote(ent.at[h], slot(h), se.at[h], re.at[h], h).wait_recv()

        cols = pl.ds(pl.multiple_of(p * C, C), C)
        lhs = lhs_of(cols)
        carried = jnp.dot(lhs, jnp.concatenate([est[p, 0], est[p, 1]], axis=1), preferred_element_type=F32)
        low_row = low_half[0:1]
        nf_row = jnp.where(low_row, esm[2 * p, 0:1], esm[2 * p + 1, 0:1])
        nb_row = jnp.where(low_row, esm[2 * p, 1:2], esm[2 * p + 1, 1:2])
        lhs32 = lhs.astype(F32)
        zf_all = jnp.sum(lhs32 * nf_row, axis=1, keepdims=True)
        zb_all = jnp.sum(lhs32 * nb_row, axis=1, keepdims=True)
        for hh in range(2):
            h = 2 * p + hh
            part = slice(hh * C, (hh + 1) * C)
            grow_f = jnp.exp(fcol[h])
            grow_b = jnp.exp(bcol[h])
            zf = zfb[h, 0:C] + grow_f * zf_all[part]
            zb = zfb[h, C:2 * C] + grow_b * zb_all[part]
            nf = nfb[h, 0:C] + grow_f * carried[part, 0:DV]
            nb = nfb[h, C:2 * C] + grow_b * carried[part, DV:2 * DV]
            total = nf / jnp.maximum(jnp.abs(zf), 1.0) + nb / jnp.maximum(jnp.abs(zb), 1.0)
            mean = jnp.mean(total * total, axis=1, keepdims=True)
            mixed = (total * lax.rsqrt(mean + EPS) * rx1[h, 1:2]).astype(BF16)
            vcols = pl.ds(pl.multiple_of(h * DV, DV), DV)
            out_ref[:, vcols] = (mixed.astype(F32) * sg[:, vcols]).astype(BF16)
        return carry

    lax.fori_loop(0, PAIRS, outer_step, 0)

    each_peer(lambda p: remote(msg_ref.at[p], rx1.at[me], sa.at[p], ra.at[me], p).wait_send())
    each_peer(lambda p: remote(lsm.at[p], rxm.at[me], sc.at[p], rc.at[me], p).wait_send())
    each_peer(lambda p: remote(lst.at[p], rxs.at[me], sb.at[p], rb.at[me], p).wait_send())
    each_peer(lambda p: remote(enm.at[p], esm.at[me], sd.at[p], rd.at[me], p).wait_send())
    each_peer(lambda p: remote(ent.at[p], slot(me), se.at[p], re.at[me], p).wait_send())


def cell(queries, keys, values, gate_logits, retention_offset, log_forget_extra, lane_amplifier, output_gate_logits):
    gates = gate_logits[0].reshape(C, H, 4).transpose(2, 1, 0).astype(F32)
    msg = jnp.concatenate(
        [
            log_forget_extra.reshape(H, 1, C),
            jnp.broadcast_to(lane_amplifier.reshape(1, 1, C), (H, 1, C)),
            jnp.broadcast_to(retention_offset.reshape(1, 2, 1), (H, 2, C)),
            jnp.zeros((H, 4, C), F32),
        ],
        axis=1,
    )
    vm = pl.BlockSpec(memory_space=pltpu.VMEM)
    dma = pltpu.SemaphoreType.DMA((H,))
    return pl.pallas_call(
        cell_kernel,
        out_shape=jax.ShapeDtypeStruct((C, H * DV), BF16),
        in_specs=[vm] * 6,
        out_specs=vm,
        scratch_shapes=[
            pltpu.VMEM((H, 8, C), F32),
            pltpu.VMEM((H, 2, DK, DV), BF16),
            pltpu.VMEM((H, 8, C), F32),
            pltpu.VMEM((H, 2, DK, DV), BF16),
            pltpu.VMEM((H, 8, C), F32),
            pltpu.VMEM((H, 2, DK, DV), BF16),
            pltpu.VMEM((H, 8, C), F32),
            pltpu.VMEM((PAIRS, 2, 2 * DK, DV), BF16),
            pltpu.VMEM((H, 8, C), F32),
            pltpu.VMEM((H, C, C), F32),
            pltpu.VMEM((H, C, C), F32),
            pltpu.VMEM((3, H, C), F32),
            pltpu.VMEM((H, 2 * C, DV), F32),
            pltpu.VMEM((H, 2 * C, C), F32),
            pltpu.VMEM((C, H * DV), F32),
        ] + [dma] * 10,
        compiler_params=pltpu.CompilerParams(
            collective_id=0, has_side_effects=True, vmem_limit_bytes=40 * 1024 * 1024),
        cost_estimate=pl.CostEstimate(flops=20_000_000_000, bytes_accessed=4_000_000, transcendentals=0),
        name="cell",
    )(queries[0], keys[0], values[0], gates, msg, output_gate_logits[0])


def on_device(
    residual_input,
    queries,
    keys,
    values,
    gate_logits,
    retention_offset,
    log_forget_extra,
    lane_amplifier,
    output_gate_logits,
    output_projection,
    cell_norm_gain,
    expert_norm_gain,
    expert_index,
    group_mixing_weight,
    within_group_weight,
    gate_weight,
    up_weight,
    down_weight,
):
    tok_rows = C
    width = residual_input.shape[2]
    gated = cell(queries, keys, values, gate_logits, retention_offset, log_forget_extra, lane_amplifier, output_gate_logits)
    proj = jnp.dot(
        gated,
        lax.all_gather(output_projection, "dp", axis=1, tiled=True),
        preferred_element_type=jnp.float32,
    )
    stream_f = residual_input.reshape(tok_rows, width).astype(jnp.float32)
    stream = (
        stream_f
        + cell_norm_gain * proj * lax.rsqrt(jnp.mean(proj * proj, axis=1, keepdims=True) + EPS)
    ).astype(jnp.bfloat16)
    stream_f = stream.astype(jnp.float32)
    moe_in = (
        expert_norm_gain
        * stream_f
        * lax.rsqrt(jnp.mean(stream_f * stream_f, axis=1, keepdims=True) + EPS)
    ).astype(jnp.bfloat16)
    seq_devices = lax.axis_size("sp")
    seq_groups = lax.axis_size("dp")
    experts = seq_devices * seq_groups
    capacity = 4 * tok_rows // experts
    flat_ids = expert_index.reshape(tok_rows * 2)
    onehot = (flat_ids[:, None] == jnp.arange(experts, dtype=jnp.int32)[None, :]).astype(jnp.int32)
    slot_index = jnp.sum((jnp.cumsum(onehot, axis=0) - onehot) * onehot, axis=1)
    target = flat_ids * capacity + slot_index
    slot_table = (
        target[:, None] == jnp.arange(experts * capacity, dtype=jnp.int32)[None, :]
    ).astype(jnp.bfloat16)
    token_table = jnp.sum(slot_table.reshape(tok_rows, 2, experts * capacity), axis=1)
    outgoing = lax.dot_general(
        token_table, moe_in, (((0,), (0,)), ((), ())), preferred_element_type=jnp.float32
    ).astype(jnp.bfloat16)
    incoming = lax.all_to_all(outgoing, ("sp", "dp"), split_axis=0, concat_axis=0, tiled=True)
    hidden = (
        jax.nn.silu(jnp.dot(incoming, gate_weight[0], preferred_element_type=jnp.float32))
        * jnp.dot(incoming, up_weight[0], preferred_element_type=jnp.float32)
    ).astype(jnp.bfloat16)
    produced = jnp.dot(hidden, down_weight[0], preferred_element_type=jnp.float32).astype(
        jnp.bfloat16
    )
    returned = lax.all_to_all(produced, ("sp", "dp"), split_axis=0, concat_axis=0, tiled=True)
    group_count = group_mixing_weight.shape[2]
    group_of = expert_index.reshape(tok_rows, 2) // (experts // group_count)
    group_hit = (
        group_of[:, :, None] == jnp.arange(group_count, dtype=jnp.int32)[None, None, :]
    ).astype(jnp.float32)
    chosen_group = jnp.sum(
        group_mixing_weight.reshape(tok_rows, 1, group_count) * group_hit, axis=2
    )
    route = chosen_group * within_group_weight.reshape(tok_rows, 2)
    picked = jnp.dot(slot_table, returned, preferred_element_type=jnp.float32).reshape(
        tok_rows, 2, width
    )
    mixture = jnp.sum(picked * route[:, :, None], axis=1)
    return (stream_f + mixture).astype(jnp.bfloat16).reshape(1, tok_rows, width)


def solution(mesh):
    in_specs = (
        P("dp", "sp", None),
        P("dp", "sp", None),
        P("dp", "sp", None),
        P("dp", "sp", None),
        P("dp", "sp", None),
        P("sp", None),
        P("dp", "sp", None),
        P("sp"),
        P("dp", "sp", None),
        P(None, "dp"),
        P(),
        P(),
        P("dp", "sp", None),
        P("dp", "sp", None),
        P("dp", "sp", None),
        P(("sp", "dp"), None, None),
        P(("sp", "dp"), None, None),
        P(("sp", "dp"), None, None),
    )
    out_specs = P("dp", "sp", None)
    return jax.shard_map(
        on_device, mesh=mesh, in_specs=in_specs, out_specs=out_specs, check_vma=False
    )
```

```python
import jax
import jax.numpy as jnp
from jax import lax
from jax.experimental import pallas as pl
from jax.experimental.pallas import tpu as pltpu
from jax.sharding import PartitionSpec as P

EPS = 1e-06
HIGH = lax.Precision.HIGHEST
F32 = jnp.float32
BF16 = jnp.bfloat16
H = 16
DK = 64
DV = 128
C = 128
D = 2048
FF = 1024
CAP = 4
DEVICES = 128
CHUNKS = 4
PER = DEVICES // CHUNKS
PAIRS = H // 2
STRIDE = 11
QUARTER = D // 4
NT = (((1,), (1,)), ((), ()))
TN = (((0,), (0,)), ((), ()))
MESH = pl.DeviceIdType.MESH


def log_sigmoid(x):
    return jnp.minimum(x, 0.0) - jnp.log1p(jnp.exp(-jnp.abs(x)))


def layer_kernel(
    q_hbm, k_hbm, v_hbm, ogl_hbm, res_hbm, wo_hbm, gate_hbm, up_hbm, down_hbm,
    g_ref, ext_ref, lam_ref, ro_ref, ids_ref, group_ref, within_ref, cng_ref, eng_ref,
    out_ref,
    q_ref, k_ref, v_ref, ogl_ref, res_ref, wbuf, gate_w, up_w, down_w,
    msg, rx1, lst, lsm, rxs, rxm, ent, enm, est, esm,
    gates, fcol, bcol, rows, nfb, zfb, sg,
    gated, proj, tab_send, tab_back, outgoing, arrived, produced, returned,
    loc, sa, ra, sb, rb, sc, rc, sd, rd, se, re,
    wsr, wsl, wrl, wrr, wps, wpr, ds, dr, bs, br,
):
    me = lax.axis_index("sp")
    dp = lax.axis_index("dp")
    z, y = lax.div(me, 4), lax.rem(me, 4)
    x, core = lax.div(dp, 2), lax.rem(dp, 2)
    flat = me * 8 + dp

    def peer_of(d):
        return lax.rem(me + d, H)

    def copy_to(src, dst, ssem, rsem, where):
        return pltpu.make_async_remote_copy(
            src_ref=src, dst_ref=dst, send_sem=ssem, recv_sem=rsem,
            device_id=where, device_id_type=MESH,
        )

    def remote(src, dst, ssem, rsem, peer):
        return copy_to(src, dst, ssem, rsem, (peer, dp))

    def each_peer(body):
        def step(d, carry):
            body(peer_of(d))
            return carry

        lax.fori_loop(1, H, step, 0)

    local = [
        pltpu.make_async_copy(src, dst, loc.at[i])
        for i, (src, dst) in enumerate((
            (wo_hbm, wbuf.at[dp]), (k_hbm, k_ref), (v_hbm, v_ref), (ogl_hbm, ogl_ref), (q_hbm, q_ref),
            (res_hbm, res_ref), (gate_hbm, gate_w), (up_hbm, up_w), (down_hbm, down_w),
        ))
    ]
    for c in local[:5]:
        c.start()

    barrier = pltpu.get_barrier_semaphore()

    def greet(d, carry):
        other = lax.rem(flat + d, DEVICES)
        pl.semaphore_signal(barrier, inc=1, device_id=(lax.div(other, 8), lax.rem(other, 8)), device_id_type=MESH)
        return carry

    lax.fori_loop(1, DEVICES, greet, 0)

    lane = lax.broadcasted_iota(jnp.int32, (C, C), 1)
    row_id = lax.broadcasted_iota(jnp.int32, (C, C), 0)
    low_half = lane < DK
    low_row = low_half[0:1]
    earlier = lane <= row_id
    diagonal = lane == row_id

    msg[:, 0, :] = ext_ref[...]
    msg[:, 1, :] = jnp.broadcast_to(lam_ref[...], (H, C))
    msg[:, 2, :] = jnp.broadcast_to(ro_ref[:, 0:1], (H, C))
    msg[:, 3, :] = jnp.broadcast_to(ro_ref[:, 1:2], (H, C))
    for i in range(4, 8):
        msg[:, i, :] = jnp.zeros((H, C), F32)
    gates[...] = g_ref[...].astype(F32)
    for c in local[:5]:
        c.wait()
    pl.semaphore_wait(barrier, DEVICES - 1)

    each_peer(lambda p: remote(msg.at[p], rx1.at[me], sa.at[p], ra.at[me], p).start())
    rx1[me] = msg[me]

    right = lax.rem(x + 1, 4) * 2 + core
    left = lax.rem(x + 3, 4) * 2 + core
    across = lax.rem(x + 2, 4) * 2 + core
    partner = x * 2 + 1 - core

    def piece(shard, i):
        return wbuf.at[shard, pl.ds(i * QUARTER, QUARTER), :]

    def to_right(shard, i, n):
        return copy_to(piece(shard, i), piece(shard, i), wsr.at[n], wrl.at[n], (me, right))

    def to_left(shard, i, n):
        return copy_to(piece(shard, i), piece(shard, i), wsl.at[n], wrr.at[n], (me, left))

    def to_partner(ref, n):
        return copy_to(ref, ref, wps.at[n], wpr.at[n], (me, partner))

    for n in range(4):
        to_right(dp, n, n).start()
        to_left(dp, (n + 2) % 4, n).start()
    to_partner(wbuf.at[dp], 0).start()
    for c in local[5:]:
        c.start()

    def gate_step(p, carry):
        cols = pl.ds(pl.multiple_of(p * 256, 256), 256)
        sg[:, cols] = 1.0 / (1.0 + jnp.exp(-ogl_ref[:, cols].astype(F32)))
        return carry

    lax.fori_loop(0, PAIRS, gate_step, 0)

    each_peer(lambda p: remote(msg.at[p], rx1.at[p], sa.at[p], ra.at[p], p).wait_recv())

    spread = rx1[:, 0, :]
    in_f = gates[pl.ds(0, H, stride=4), :]
    in_b = gates[pl.ds(2, H, stride=4), :]
    fade_f = log_sigmoid(gates[pl.ds(1, H, stride=4), :] + rx1[:, 2, :]) + spread
    fade_b = log_sigmoid(gates[pl.ds(3, H, stride=4), :] + rx1[:, 3, :]) + spread
    upto = (row_id <= lane).astype(F32)
    since = (row_id >= lane).astype(F32)
    cum_f = jnp.dot(fade_f, upto, precision=HIGH, preferred_element_type=F32)
    cum_b = jnp.dot(fade_b, since, precision=HIGH, preferred_element_type=F32)
    end_f = jnp.broadcast_to(cum_f[:, C - 1:C], (H, C))
    end_b = jnp.broadcast_to(cum_b[:, 0:1], (H, C))
    w_f = jnp.exp(end_f - cum_f + in_f)
    w_b = jnp.exp(end_b - cum_b + in_b)
    rows[0] = cum_f - in_f
    rows[1] = cum_b - in_b
    rows[2] = jnp.exp(in_b)
    turned = jnp.concatenate([cum_f, cum_b, w_f, w_b, jnp.zeros((C - 4 * H, C), F32)], axis=0).T
    wf_hi = w_f.astype(BF16)
    wb_hi = w_b.astype(BF16)
    wf_lo = (w_f - wf_hi.astype(F32)).astype(BF16)
    wb_lo = (w_b - wb_hi.astype(F32)).astype(BF16)
    stacked = jnp.concatenate([wf_hi, wf_lo, wb_hi, wb_lo], axis=0)
    for p in range(PAIRS):
        kp = k_ref[:, p * C:(p + 1) * C]
        k32 = kp.astype(F32)
        h0, h1 = 2 * p, 2 * p + 1
        wf = jnp.where(low_half, turned[:, 32 + h0:33 + h0], turned[:, 32 + h1:33 + h1])
        wb = jnp.where(low_half, turned[:, 48 + h0:49 + h0], turned[:, 48 + h1:49 + h1])
        both = jnp.concatenate([k32 * wf, k32 * wb], axis=1).astype(BF16)
        state = lax.dot_general(both, v_ref[:, p * 256:(p + 1) * 256], TN, preferred_element_type=F32).astype(BF16)
        lst[h0, 0] = state[0:64, 0:128]
        lst[h1, 0] = state[64:128, 128:256]
        lst[h0, 1] = state[128:192, 0:128]
        lst[h1, 1] = state[192:256, 128:256]
        norm = jnp.dot(stacked, kp, preferred_element_type=F32)
        norm_f = norm[0:16] + norm[16:32]
        norm_b = norm[32:48] + norm[48:64]
        for h, keep in ((h0, low_row), (h1, ~low_row)):
            nf = norm_f[h:h + 1]
            nb = norm_b[h:h + 1]
            nf = jnp.where(keep, nf, pltpu.roll(nf, DK, 1))
            nb = jnp.where(keep, nb, pltpu.roll(nb, DK, 1))
            lsm[h] = jnp.concatenate(
                [nf, nb, end_f[h:h + 1], end_b[h:h + 1], jnp.zeros((4, C), F32)], axis=0)

    each_peer(lambda p: remote(lsm.at[p], rxm.at[me], sc.at[p], rc.at[me], p).start())
    each_peer(lambda p: remote(lst.at[p], rxs.at[me], sb.at[p], rb.at[me], p).start())
    rxs[me] = lst[me]
    rxm[me] = lsm[me]

    for h in range(H):
        fcol[h] = jnp.broadcast_to(turned[:, h:h + 1], (C, C))
        bcol[h] = jnp.broadcast_to(turned[:, 16 + h:17 + h], (C, C))

    def lhs_of(cols):
        qp = q_ref[:, cols] * jnp.asarray(DK ** -0.5, BF16)
        none = jnp.zeros_like(qp)
        return jnp.concatenate([jnp.where(low_half, qp, none), jnp.where(low_half, none, qp)], axis=0)

    def inner_step(p, carry):
        cols = pl.ds(pl.multiple_of(p * C, C), C)
        score2 = lax.dot_general(lhs_of(cols), k_ref[:, cols], NT, preferred_element_type=F32)
        for hh in range(2):
            h = 2 * p + hh
            score = score2[hh * C:(hh + 1) * C]
            ahead = fcol[h] - rows[0, pl.ds(h, 1), :]
            behind = bcol[h] - rows[1, pl.ds(h, 1), :]
            weighted = score * jnp.exp(jnp.where(earlier, ahead, behind))
            pf = jnp.where(earlier, weighted, 0.0)
            pb = jnp.where(earlier, jnp.where(diagonal, score * rows[2, pl.ds(h, 1), :], 0.0), weighted)
            both = jnp.concatenate([pf, pb], axis=0)
            zfb[h] = jnp.broadcast_to(jnp.sum(both, axis=1, keepdims=True), (2 * C, C))
            vcols = pl.ds(pl.multiple_of(h * DV, DV), DV)
            nfb[h] = jnp.dot(both.astype(BF16), v_ref[:, vcols], preferred_element_type=F32)
        return carry

    lax.fori_loop(0, PAIRS, inner_step, 0)

    each_peer(lambda p: remote(lsm.at[p], rxm.at[p], sc.at[p], rc.at[p], p).wait_recv())
    each_peer(lambda p: remote(lst.at[p], rxs.at[p], sb.at[p], rb.at[p], p).wait_recv())

    enm[...] = jnp.zeros_like(enm)

    def carry_step(c, state):
        mf, mb, nf, nb = state
        d = H - 1 - c
        ent[c, 0] = mf.astype(BF16)
        ent[d, 1] = mb.astype(BF16)
        enm[c, 0:1] = nf
        enm[d, 1:2] = nb
        keep_f = jnp.exp(rxm[c, 2:3])
        keep_b = jnp.exp(rxm[d, 3:4])
        return (
            mf * keep_f + rxs[c, 0].astype(F32),
            mb * keep_b + rxs[d, 1].astype(F32),
            nf * keep_f + rxm[c, 0:1],
            nb * keep_b + rxm[d, 1:2],
        )

    zero_m = jnp.zeros((DK, DV), F32)
    zero_n = jnp.zeros((1, C), F32)
    lax.fori_loop(0, H, carry_step, (zero_m, zero_m, zero_n, zero_n))

    def slot(h):
        return est.at[lax.div(h, 2), :, pl.ds(pl.multiple_of(lax.rem(h, 2) * DK, DK), DK), :]

    each_peer(lambda p: remote(enm.at[p], esm.at[me], sd.at[p], rd.at[me], p).start())
    each_peer(lambda p: remote(ent.at[p], slot(me), se.at[p], re.at[me], p).start())
    esm[me] = enm[me]
    est[lax.div(me, 2), :, pl.ds(pl.multiple_of(lax.rem(me, 2) * DK, DK), DK), :] = ent[me]

    for n in range(2):
        to_right(left, n, n).wait_recv()
        to_right(left, n, 4 + n).start()
        to_left(right, n + 2, n).wait_recv()
        to_left(right, n + 2, 4 + n).start()

    table_in = jnp.concatenate(
        [ids_ref[...].astype(F32), group_ref[...], within_ref[...], jnp.zeros((C - 8, C), F32)], axis=0).T
    wide = lax.broadcasted_iota(jnp.int32, (C, DEVICES * CAP), 1)
    hits, targets, routes = [], [], []
    for n in range(2):
        expert = table_in[:, n:n + 1].astype(jnp.int32)
        dz = jnp.bitwise_and(jnp.right_shift(expert, 5) - z + 4, 3)
        dy = jnp.bitwise_and(jnp.right_shift(expert, 3) - y + 8, 3)
        dx = jnp.bitwise_and(jnp.right_shift(expert, 1) - x + 4, 3)
        dc = jnp.bitwise_and(expert - core + 2, 1)
        place = jnp.bitwise_and(dz + dy + dx, 3) * PER + dy * 8 + dx * 2 + dc
        group = jnp.right_shift(expert, 5)
        share = jnp.zeros((C, 1), F32)
        for i in range(4):
            share = share + jnp.where(group == i, table_in[:, 2 + i:3 + i], 0.0)
        routes.append(share * table_in[:, 6 + n:7 + n])
        targets.append(place * CAP)
        hits.append((lane == place).astype(F32))
    before = jnp.dot((lane < row_id).astype(BF16), (hits[0] + hits[1]).astype(BF16), preferred_element_type=F32)
    sent = jnp.zeros((C, DEVICES * CAP), F32)
    back = jnp.zeros((C, DEVICES * CAP), F32)
    for n in range(2):
        nth = jnp.sum(before * hits[n], axis=1, keepdims=True).astype(jnp.int32)
        chosen = wide == targets[n] + nth
        sent = sent + jnp.where(chosen, 1.0, 0.0)
        back = back + jnp.where(chosen, routes[n], 0.0)
    tab_send[...] = sent.astype(BF16)
    back_hi = back.astype(BF16)
    tab_back[0:C] = back_hi
    tab_back[C:2 * C] = (back - back_hi.astype(F32)).astype(BF16)

    def outer_step(p, carry):
        for hh in range(2):
            h = 2 * p + hh

            @pl.when(h != me)
            def _():
                remote(enm.at[h], esm.at[h], sd.at[h], rd.at[h], h).wait_recv()
                remote(ent.at[h], slot(h), se.at[h], re.at[h], h).wait_recv()

        cols = pl.ds(pl.multiple_of(p * C, C), C)
        lhs = lhs_of(cols)
        carried = jnp.dot(lhs, jnp.concatenate([est[p, 0], est[p, 1]], axis=1), preferred_element_type=F32)
        nf_row = jnp.where(low_row, esm[2 * p, 0:1], esm[2 * p + 1, 0:1])
        nb_row = jnp.where(low_row, esm[2 * p, 1:2], esm[2 * p + 1, 1:2])
        lhs32 = lhs.astype(F32)
        zf_all = jnp.sum(lhs32 * nf_row, axis=1, keepdims=True)
        zb_all = jnp.sum(lhs32 * nb_row, axis=1, keepdims=True)
        for hh in range(2):
            h = 2 * p + hh
            part = slice(hh * C, (hh + 1) * C)
            grow_f = jnp.exp(fcol[h])
            grow_b = jnp.exp(bcol[h])
            zf = zfb[h, 0:C] + grow_f * zf_all[part]
            zb = zfb[h, C:2 * C] + grow_b * zb_all[part]
            nf = nfb[h, 0:C] + grow_f * carried[part, 0:DV]
            nb = nfb[h, C:2 * C] + grow_b * carried[part, DV:2 * DV]
            total = nf / jnp.maximum(jnp.abs(zf), 1.0) + nb / jnp.maximum(jnp.abs(zb), 1.0)
            mean = jnp.mean(total * total, axis=1, keepdims=True)
            mixed = (total * lax.rsqrt(mean + EPS) * rx1[h, 1:2]).astype(BF16)
            vcols = pl.ds(pl.multiple_of(h * DV, DV), DV)
            gated[:, vcols] = (mixed.astype(F32) * sg[:, vcols]).astype(BF16)
        return carry

    lax.fori_loop(0, PAIRS, outer_step, 0)

    def project(shard):
        cols = pl.ds(pl.multiple_of(shard * 256, 256), 256)
        proj[:, cols] = jnp.dot(gated[...], wbuf[shard], preferred_element_type=F32)

    project(dp)
    for n in range(2, 4):
        to_right(left, n, n).wait_recv()
        to_left(right, n - 2, n).wait_recv()
    to_partner(wbuf.at[left], 1).start()
    to_partner(wbuf.at[right], 2).start()
    project(left)
    project(right)
    far = 1 - 2 * core
    to_partner(wbuf.at[partner], 0).wait_recv()
    project(partner)
    for n in range(2):
        to_right(across, n, 4 + n).wait_recv()
        to_partner(piece(across, n), 3 + n).start()
        to_left(across, n + 2, 4 + n).wait_recv()
        to_partner(piece(across, n + 2), 5 + n).start()
    to_partner(wbuf.at[left + far], 1).wait_recv()
    project(left + far)
    to_partner(wbuf.at[right + far], 2).wait_recv()
    project(right + far)
    project(across)
    for n in range(2):
        to_partner(piece(across + far, n), 3 + n).wait_recv()
        to_partner(piece(across + far, n + 2), 5 + n).wait_recv()
    project(across + far)

    local[5].wait()
    pr = proj[...]
    scale = lax.rsqrt(jnp.mean(pr * pr, axis=1, keepdims=True) + EPS)
    stream = (res_ref[...].astype(F32) + cng_ref[...] * pr * scale).astype(BF16).astype(F32)
    proj[...] = stream
    scale = lax.rsqrt(jnp.mean(stream * stream, axis=1, keepdims=True) + EPS)
    gated[...] = (eng_ref[...] * stream * scale).astype(BF16)

    def route_of(j, i):
        t = lax.rem(i * STRIDE, PER)
        dc = lax.rem(t, 2)
        dx = lax.rem(lax.div(t, 2), 4)
        dy = lax.div(t, 8)
        dz = lax.rem(j + 8 - dx - dy, 4)
        return j * PER + t, dz, dy, dx, dc

    def onward(j, i):
        place, dz, dy, dx, dc = route_of(j, i)
        sp_to = lax.rem(z + dz, 4) * 4 + lax.rem(y + dy, 4)
        dp_to = lax.rem(x + dx, 4) * 2 + lax.rem(core + dc, 2)
        return place, (sp_to, dp_to)

    def homeward(j, i):
        place, dz, dy, dx, dc = route_of(j, i)
        sp_to = lax.rem(z + 4 - dz, 4) * 4 + lax.rem(y + 4 - dy, 4)
        dp_to = lax.rem(x + 4 - dx, 4) * 2 + lax.rem(core + dc, 2)
        return place, (sp_to, dp_to)

    def send_chunk(j, way, src, dst, ssem, rsem):
        def step(i, carry):
            place, where = way(j, i)

            @pl.when(place != 0)
            def _():
                copy_to(src.at[place], dst.at[place], ssem.at[j], rsem.at[j], where).start()

            return carry

        lax.fori_loop(0, PER, step, 0)

    def whole(j, src, dst, ssem, rsem):
        span = pl.ds(1, PER - 1) if j == 0 else pl.ds(j * PER, PER)
        return copy_to(src.at[span], dst.at[span], ssem.at[j], rsem.at[j], (me, partner))

    for j in range(CHUNKS):
        rows_out = lax.dot_general(
            tab_send[:, j * C:(j + 1) * C], gated[...], TN, preferred_element_type=F32)
        outgoing[j * PER:(j + 1) * PER] = rows_out.astype(BF16).reshape(PER, CAP, D)
        send_chunk(j, onward, outgoing, arrived, ds, dr)
        if j == 0:
            arrived[0] = outgoing[0]

    for c in local[6:]:
        c.wait()

    def expert_chunk(j):
        rows_in = arrived[pl.ds(j * PER, PER)].reshape(PER * CAP, D)
        a = jnp.dot(rows_in, gate_w[...], preferred_element_type=F32)
        b = jnp.dot(rows_in, up_w[...], preferred_element_type=F32)
        hidden = (a / (1.0 + jnp.exp(-a)) * b).astype(BF16)
        made = jnp.dot(hidden, down_w[...], preferred_element_type=F32).astype(BF16)
        produced[pl.ds(j * PER, PER)] = made.reshape(PER, CAP, D)

    def expert_step(j, carry):
        for n in range(CHUNKS):
            @pl.when(j == n)
            def _():
                whole(n, outgoing, arrived, ds, dr).wait_recv()

        expert_chunk(j)
        send_chunk(j, homeward, produced, returned, bs, br)
        return carry

    lax.fori_loop(0, CHUNKS, expert_step, 0)
    returned[0] = produced[0]

    for j in range(CHUNKS):
        whole(j, produced, returned, bs, br).wait_recv()
        rows_back = returned[j * PER:(j + 1) * PER].reshape(PER * CAP, D)
        parts = jnp.dot(tab_back[:, j * C:(j + 1) * C], rows_back, preferred_element_type=F32)
        proj[...] += parts[0:C] + parts[C:2 * C]
    out_ref[...] = proj[...].astype(BF16)

    each_peer(lambda p: remote(msg.at[p], rx1.at[me], sa.at[p], ra.at[me], p).wait_send())
    each_peer(lambda p: remote(lsm.at[p], rxm.at[me], sc.at[p], rc.at[me], p).wait_send())
    each_peer(lambda p: remote(lst.at[p], rxs.at[me], sb.at[p], rb.at[me], p).wait_send())
    each_peer(lambda p: remote(enm.at[p], esm.at[me], sd.at[p], rd.at[me], p).wait_send())
    each_peer(lambda p: remote(ent.at[p], slot(me), se.at[p], re.at[me], p).wait_send())
    for n in range(6):
        to_right(dp, 0, n).wait_send()
        to_left(dp, 0, n).wait_send()
    for n in range(3):
        to_partner(wbuf.at[dp], n).wait_send()
    for n in range(3, 7):
        to_partner(piece(dp, 0), n).wait_send()
    for j in range(CHUNKS):
        whole(j, outgoing, arrived, ds, dr).wait_send()
        whole(j, produced, returned, bs, br).wait_send()


def on_device(
    residual_input, queries, keys, values, gate_logits, retention_offset, log_forget_extra,
    lane_amplifier, output_gate_logits, output_projection, cell_norm_gain, expert_norm_gain,
    expert_index, group_mixing_weight, within_group_weight, gate_weight, up_weight, down_weight,
):
    vm = pl.BlockSpec(memory_space=pltpu.VMEM)
    hbm = pl.BlockSpec(memory_space=pl.ANY)
    dma = pltpu.SemaphoreType.DMA
    small = pltpu.VMEM((H, 8, C), F32)
    state = pltpu.VMEM((H, 2, DK, DV), BF16)
    slots = pltpu.VMEM((DEVICES, CAP, D), BF16)
    out = pl.pallas_call(
        layer_kernel,
        out_shape=jax.ShapeDtypeStruct((C, D), BF16),
        in_specs=[hbm] * 9 + [vm] * 9,
        out_specs=vm,
        scratch_shapes=[
            pltpu.VMEM((C, H * DK), BF16),
            pltpu.VMEM((C, H * DK), BF16),
            pltpu.VMEM((C, H * DV), BF16),
            pltpu.VMEM((C, H * DV), BF16),
            pltpu.VMEM((C, D), BF16),
            pltpu.VMEM((8, D, 256), BF16),
            pltpu.VMEM((D, FF), BF16),
            pltpu.VMEM((D, FF), BF16),
            pltpu.VMEM((FF, D), BF16),
            small, small, state, small, state, small, state, small,
            pltpu.VMEM((PAIRS, 2, 2 * DK, DV), BF16),
            small,
            pltpu.VMEM((4 * H, C), F32),
            pltpu.VMEM((H, C, C), F32),
            pltpu.VMEM((H, C, C), F32),
            pltpu.VMEM((3, H, C), F32),
            pltpu.VMEM((H, 2 * C, DV), F32),
            pltpu.VMEM((H, 2 * C, C), F32),
            pltpu.VMEM((C, H * DV), F32),
            pltpu.VMEM((C, H * DV), BF16),
            pltpu.VMEM((C, D), F32),
            pltpu.VMEM((C, DEVICES * CAP), BF16),
            pltpu.VMEM((2 * C, DEVICES * CAP), BF16),
            slots, slots, slots, slots,
            dma((9,)),
        ] + [dma((H,))] * 10 + [dma((6,))] * 4 + [dma((7,))] * 2 + [dma((CHUNKS,))] * 4,
        compiler_params=pltpu.CompilerParams(
            collective_id=0, has_side_effects=True, vmem_limit_bytes=67_043_328),
        name="layer",
    )(
        queries[0], keys[0], values[0], output_gate_logits[0], residual_input[0], output_projection,
        gate_weight[0], up_weight[0], down_weight[0],
        gate_logits[0].T, log_forget_extra.reshape(H, C), lane_amplifier.reshape(1, C), retention_offset,
        expert_index[0].T, group_mixing_weight[0].T, within_group_weight[0].T,
        cell_norm_gain.reshape(1, D), expert_norm_gain.reshape(1, D),
    )
    return out.reshape(1, C, D)


def solution(mesh):
    by_place = P("dp", "sp", None)
    by_expert = P(("sp", "dp"), None, None)
    in_specs = (
        by_place, by_place, by_place, by_place, by_place, P("sp", None), by_place, P("sp"), by_place,
        P(None, "dp"), P(), P(), by_place, by_place, by_place, by_expert, by_expert, by_expert,
    )
    return jax.shard_map(on_device, mesh=mesh, in_specs=in_specs, out_specs=by_place, check_vma=False)
```

```python
import jax
import jax.numpy as jnp
from jax import lax
from jax.experimental import pallas as pl
from jax.experimental.pallas import tpu as pltpu
from jax.sharding import PartitionSpec as P

EPS = 1e-06
HIGH = lax.Precision.HIGHEST
F32 = jnp.float32
BF16 = jnp.bfloat16
H = 16
DK = 64
DV = 128
C = 128
D = 2048
FF = 1024
CAP = 4
DEVICES = 128
CHUNKS = 4
PER = DEVICES // CHUNKS
PAIRS = H // 2
STRIDE = 11
PIECE = 32
BASE = H * PIECE
QUARTER = (D - BASE) // 4
NT = (((1,), (1,)), ((), ()))
TN = (((0,), (0,)), ((), ()))
MESH = pl.DeviceIdType.MESH


def log_sigmoid(x):
    return jnp.minimum(x, 0.0) - jnp.log1p(jnp.exp(-jnp.abs(x)))


def layer_kernel(
    q_hbm, k_hbm, v_hbm, ogl_hbm, res_hbm, wo_hbm, gate_hbm, up_hbm, down_hbm,
    g_hbm, ext_hbm, lam_hbm, ro_hbm, ids_hbm, group_hbm, within_hbm, cng_hbm, eng_hbm,
    out_ref,
    g_ref, ext_ref, lam_ref, ro_ref, ids_ref, group_ref, within_ref, cng_ref, eng_ref,
    q_ref, k_ref, v_ref, ogl_ref, res_ref, wbuf, gate_w, up_w, down_w,
    msg, rx1, lst, lsm, rxs, rxm, ent, enm, est, esm,
    gates, fcol, bcol, rows, wpair, nfb, zfb, sg,
    gated, proj, tab_send, tab_back, outgoing, arrived, produced, returned,
    loc, sa, ra, sb, rb, sbb, rbb, sc, rc, sd, rd, se, re, seb, reb,
    wsr, wsl, wrl, wrr, wps, wpr, pxs, pxr, pys, pyr, ds, dr, bs, br, meet,
):
    me = lax.axis_index("sp")
    dp = lax.axis_index("dp")
    z, y = lax.div(me, 4), lax.rem(me, 4)
    x, core = lax.div(dp, 2), lax.rem(dp, 2)
    flat = me * 8 + dp

    def peer_of(d):
        return lax.rem(me + d, H)

    def copy_to(src, dst, ssem, rsem, where):
        return pltpu.make_async_remote_copy(
            src_ref=src, dst_ref=dst, send_sem=ssem, recv_sem=rsem,
            device_id=where, device_id_type=MESH,
        )

    def remote(src, dst, ssem, rsem, peer):
        return copy_to(src, dst, ssem, rsem, (peer, dp))

    def each_peer(body):
        def step(d, carry):
            body(peer_of(d))
            return carry

        lax.fori_loop(1, H, step, 0)

    barrier = pltpu.get_barrier_semaphore()

    def greet(where):
        pl.semaphore_signal(barrier, inc=1, device_id=where, device_id_type=MESH)

    each_peer(lambda p: greet((p, dp)))
    for n in range(1, 8):
        greet((me, lax.rem(dp + n, 8)))

    local = [
        pltpu.make_async_copy(src, dst, loc.at[i])
        for i, (src, dst) in enumerate((
            (ext_hbm, ext_ref), (lam_hbm, lam_ref), (ro_hbm, ro_ref), (g_hbm, g_ref),
            (wo_hbm, wbuf.at[dp]), (k_hbm, k_ref), (v_hbm, v_ref), (q_hbm, q_ref), (ogl_hbm, ogl_ref),
            (ids_hbm, ids_ref), (group_hbm, group_ref), (within_hbm, within_ref),
            (cng_hbm, cng_ref), (eng_hbm, eng_ref),
            (res_hbm, res_ref), (gate_hbm, gate_w), (up_hbm, up_w), (down_hbm, down_w),
        ))
    ]
    for c in local[:14]:
        c.start()

    lane = lax.broadcasted_iota(jnp.int32, (C, C), 1)
    row_id = lax.broadcasted_iota(jnp.int32, (C, C), 0)
    low_half = lane < DK
    low_row = low_half[0:1]
    earlier = lane <= row_id
    diagonal = lane == row_id

    for c in local[:4]:
        c.wait()
    msg[:, 0, :] = ext_ref[...]
    msg[:, 1, :] = jnp.broadcast_to(lam_ref[...], (H, C))
    msg[:, 2, :] = jnp.broadcast_to(ro_ref[:, 0:1], (H, C))
    msg[:, 3, :] = jnp.broadcast_to(ro_ref[:, 1:2], (H, C))
    for i in range(4, 8):
        msg[:, i, :] = jnp.zeros((H, C), F32)
    gates[...] = g_ref[...].astype(F32)
    pl.semaphore_wait(barrier, H - 1 + 7)

    each_peer(lambda p: remote(msg.at[p], rx1.at[me], sa.at[p], ra.at[me], p).start())
    rx1[me] = msg[me]

    right = lax.rem(x + 1, 4) * 2 + core
    left = lax.rem(x + 3, 4) * 2 + core
    across = lax.rem(x + 2, 4) * 2 + core
    partner = x * 2 + 1 - core

    def piece(shard, i):
        return wbuf.at[shard, pl.ds(BASE + i * QUARTER, QUARTER), :]

    def strip(shard, owner):
        return wbuf.at[shard, pl.ds(pl.multiple_of(owner * PIECE, PIECE), PIECE), :]

    others = ((right, left), (left, right), (across, across))

    def strip_out(n):
        ref = strip(dp, me)
        return copy_to(ref, ref, pxs.at[n], pxr.at[n], (me, others[n][0]))

    def strip_on(n, peer):
        ref = strip(others[n][1], me)
        return copy_to(ref, ref, pys.at[n], pyr.at[n], (peer, dp))

    def strips(n):
        ref = wbuf.at[others[n][1], pl.ds(0, BASE - PIECE), :]
        return copy_to(ref, ref, pys.at[n], pyr.at[n], (me, partner))

    def pass_strip(n):
        strip_out(n).wait_recv()
        each_peer(lambda p: strip_on(n, p).start())

    def to_right(shard, i, n):
        return copy_to(piece(shard, i), piece(shard, i), wsr.at[n], wrl.at[n], (me, right))

    def to_left(shard, i, n):
        return copy_to(piece(shard, i), piece(shard, i), wsl.at[n], wrr.at[n], (me, left))

    def to_partner(ref, n):
        return copy_to(ref, ref, wps.at[n], wpr.at[n], (me, partner))

    local[4].wait()
    for n in range(3):
        strip_out(n).start()
    for n in range(4):
        to_right(dp, n, n).start()
        to_left(dp, (n + 2) % 4, n).start()
    to_partner(wbuf.at[dp], 0).start()
    for c in local[5:14]:
        c.wait()
    for c in local[14:]:
        c.start()

    def gate_step(p, carry):
        cols = pl.ds(pl.multiple_of(p * 256, 256), 256)
        sg[:, cols] = 1.0 / (1.0 + jnp.exp(-ogl_ref[:, cols].astype(F32)))
        return carry

    lax.fori_loop(0, PAIRS, gate_step, 0)

    pass_strip(0)
    table_in = jnp.concatenate(
        [ids_ref[...].astype(F32), group_ref[...], within_ref[...], jnp.zeros((C - 8, C), F32)], axis=0).T
    wide = lax.broadcasted_iota(jnp.int32, (C, DEVICES * CAP), 1)
    hits, targets, routes = [], [], []
    for n in range(2):
        expert = table_in[:, n:n + 1].astype(jnp.int32)
        dz = jnp.bitwise_and(jnp.right_shift(expert, 5) - z + 4, 3)
        dy = jnp.bitwise_and(jnp.right_shift(expert, 3) - y + 8, 3)
        dx = jnp.bitwise_and(jnp.right_shift(expert, 1) - x + 4, 3)
        dc = jnp.bitwise_and(expert - core + 2, 1)
        place = jnp.bitwise_and(dz + dy + dx, 3) * PER + dy * 8 + dx * 2 + dc
        group = jnp.right_shift(expert, 5)
        share = jnp.zeros((C, 1), F32)
        for i in range(4):
            share = share + jnp.where(group == i, table_in[:, 2 + i:3 + i], 0.0)
        routes.append(share * table_in[:, 6 + n:7 + n])
        targets.append(place * CAP)
        hits.append((lane == place).astype(F32))
    before = jnp.dot((lane < row_id).astype(BF16), (hits[0] + hits[1]).astype(BF16), preferred_element_type=F32)
    sent = jnp.zeros((C, DEVICES * CAP), F32)
    back = jnp.zeros((C, DEVICES * CAP), F32)
    for n in range(2):
        nth = jnp.sum(before * hits[n], axis=1, keepdims=True).astype(jnp.int32)
        chosen = wide == targets[n] + nth
        sent = sent + jnp.where(chosen, 1.0, 0.0)
        back = back + jnp.where(chosen, routes[n], 0.0)
    tab_send[...] = sent.astype(BF16)
    back_hi = back.astype(BF16)
    tab_back[0:C] = back_hi
    tab_back[C:2 * C] = (back - back_hi.astype(F32)).astype(BF16)

    each_peer(lambda p: remote(msg.at[p], rx1.at[p], sa.at[p], ra.at[p], p).wait_recv())

    spread = rx1[:, 0, :]
    in_f = gates[pl.ds(0, H, stride=4), :]
    in_b = gates[pl.ds(2, H, stride=4), :]
    fade_f = log_sigmoid(gates[pl.ds(1, H, stride=4), :] + rx1[:, 2, :]) + spread
    fade_b = log_sigmoid(gates[pl.ds(3, H, stride=4), :] + rx1[:, 3, :]) + spread
    upto = (row_id <= lane).astype(F32)
    since = (row_id >= lane).astype(F32)
    cum_f = jnp.dot(fade_f, upto, precision=HIGH, preferred_element_type=F32)
    cum_b = jnp.dot(fade_b, since, precision=HIGH, preferred_element_type=F32)
    end_f = jnp.broadcast_to(cum_f[:, C - 1:C], (H, C))
    end_b = jnp.broadcast_to(cum_b[:, 0:1], (H, C))
    w_f = jnp.exp(end_f - cum_f + in_f)
    w_b = jnp.exp(end_b - cum_b + in_b)
    rows[0] = cum_f - in_f
    rows[1] = cum_b - in_b
    rows[2] = jnp.exp(in_b)
    turned = jnp.concatenate([cum_f, cum_b, w_f, w_b, jnp.zeros((C - 4 * H, C), F32)], axis=0).T
    wf_hi = w_f.astype(BF16)
    wb_hi = w_b.astype(BF16)
    wf_lo = (w_f - wf_hi.astype(F32)).astype(BF16)
    wb_lo = (w_b - wb_hi.astype(F32)).astype(BF16)
    stacked = jnp.concatenate([wf_hi, wf_lo, wb_hi, wb_lo], axis=0)
    norm = jnp.dot(stacked, k_ref[...], preferred_element_type=F32)
    norm_f = norm[0:16] + norm[16:32]
    norm_b = norm[32:48] + norm[48:64]
    for p in range(PAIRS):
        h0, h1 = 2 * p, 2 * p + 1
        wpair[p, 0] = jnp.where(low_half, turned[:, 32 + h0:33 + h0], turned[:, 32 + h1:33 + h1])
        wpair[p, 1] = jnp.where(low_half, turned[:, 48 + h0:49 + h0], turned[:, 48 + h1:49 + h1])
        for h, keep in ((h0, low_row), (h1, ~low_row)):
            nf = norm_f[h:h + 1, p * C:(p + 1) * C]
            nb = norm_b[h:h + 1, p * C:(p + 1) * C]
            nf = jnp.where(keep, nf, pltpu.roll(nf, DK, 1))
            nb = jnp.where(keep, nb, pltpu.roll(nb, DK, 1))
            lsm[h] = jnp.concatenate(
                [nf, nb, end_f[h:h + 1], end_b[h:h + 1], jnp.zeros((4, C), F32)], axis=0)

    each_peer(lambda p: remote(lsm.at[p], rxm.at[me], sc.at[p], rc.at[me], p).start())
    rxm[me] = lsm[me]
    first = lax.div(me, 2) + 1

    def state_out(way, h, ssem, rsem):
        return remote(lst.at[h, way], rxs.at[me, way], ssem.at[h], rsem.at[me], h)

    def state_in(way, h, ssem, rsem):
        return remote(lst.at[h, way], rxs.at[h, way], ssem.at[h], rsem.at[h], h)

    def post_pair(i):
        p = lax.rem(first + i, PAIRS)
        for hh in range(2):
            h = 2 * p + hh

            @pl.when(h != me)
            def _():
                state_out(0, h, sb, rb).start()

    def state_step(i, carry):
        p = lax.rem(first + i, PAIRS)
        k32 = k_ref[:, pl.ds(pl.multiple_of(p * C, C), C)].astype(F32)
        both = jnp.concatenate([k32 * wpair[p, 0], k32 * wpair[p, 1]], axis=1).astype(BF16)
        vp = v_ref[:, pl.ds(pl.multiple_of(p * 256, 256), 256)]
        state = lax.dot_general(both, vp, TN, preferred_element_type=F32).astype(BF16)
        lst[2 * p, 0] = state[0:64, 0:128]
        lst[2 * p + 1, 0] = state[64:128, 128:256]
        lst[2 * p, 1] = state[128:192, 0:128]
        lst[2 * p + 1, 1] = state[192:256, 128:256]

        @pl.when(i > 0)
        def _():
            post_pair(i - 1)

        return carry

    lax.fori_loop(0, PAIRS, state_step, 0)
    post_pair(PAIRS - 1)
    each_peer(lambda p: state_out(1, p, sbb, rbb).start())
    rxs[me] = lst[me]

    def relay(n):
        to_right(left, n, n).wait_recv()
        to_right(left, n, 4 + n).start()
        to_left(right, n + 2, n).wait_recv()
        to_left(right, n + 2, 4 + n).start()


    for h in range(H):
        fcol[h] = jnp.broadcast_to(turned[:, h:h + 1], (C, C))
        bcol[h] = jnp.broadcast_to(turned[:, 16 + h:17 + h], (C, C))

    relay(0)

    def lhs_of(cols):
        qp = q_ref[:, cols] * jnp.asarray(DK ** -0.5, BF16)
        none = jnp.zeros_like(qp)
        return jnp.concatenate([jnp.where(low_half, qp, none), jnp.where(low_half, none, qp)], axis=0)

    def inner_step(p, carry):
        cols = pl.ds(pl.multiple_of(p * C, C), C)
        score2 = lax.dot_general(lhs_of(cols), k_ref[:, cols], NT, preferred_element_type=F32)
        for hh in range(2):
            h = 2 * p + hh
            score = score2[hh * C:(hh + 1) * C]
            ahead = fcol[h] - rows[0, pl.ds(h, 1), :]
            behind = bcol[h] - rows[1, pl.ds(h, 1), :]
            weighted = score * jnp.exp(jnp.where(earlier, ahead, behind))
            pf = jnp.where(earlier, weighted, 0.0)
            pb = jnp.where(earlier, jnp.where(diagonal, score * rows[2, pl.ds(h, 1), :], 0.0), weighted)
            both = jnp.concatenate([pf, pb], axis=0)
            zfb[h] = jnp.broadcast_to(jnp.sum(both, axis=1, keepdims=True), (2 * C, C))
            vcols = pl.ds(pl.multiple_of(h * DV, DV), DV)
            nfb[h] = jnp.dot(both.astype(BF16), v_ref[:, vcols], preferred_element_type=F32)
        return carry

    lax.fori_loop(0, PAIRS, inner_step, 0)

    relay(1)
    each_peer(lambda p: remote(lsm.at[p], rxm.at[p], sc.at[p], rc.at[p], p).wait_recv())
    enm[...] = jnp.zeros_like(enm)

    def slot(way, h):
        return est.at[lax.div(h, 2), way, pl.ds(pl.multiple_of(lax.rem(h, 2) * DK, DK), DK), :]

    def entry_out(way, p, ssem, rsem):
        return remote(ent.at[p, way], slot(way, me), ssem.at[p], rsem.at[me], p)

    def entry_in(way, p, ssem, rsem):
        return remote(ent.at[p, way], slot(way, p), ssem.at[p], rsem.at[p], p)

    def run(way, ssem, rsem, ssem_out, rsem_out):
        each_peer(lambda p: state_in(way, p, ssem, rsem).wait_recv())

        def carry_step(i, state):
            m, n = state
            c = i if way == 0 else H - 1 - i
            ent[c, way] = m.astype(BF16)
            enm[c, way:way + 1] = n
            keep = jnp.exp(rxm[c, 2 + way:3 + way])
            return m * keep + rxs[c, way].astype(F32), n * keep + rxm[c, way:way + 1]

        lax.fori_loop(0, H, carry_step, (jnp.zeros((DK, DV), F32), jnp.zeros((1, C), F32)))
        each_peer(lambda p: entry_out(way, p, ssem_out, rsem_out).start())

    run(0, sb, rb, se, re)
    run(1, sbb, rbb, seb, reb)
    each_peer(lambda p: remote(enm.at[p], esm.at[me], sd.at[p], rd.at[me], p).start())
    esm[me] = enm[me]
    est[lax.div(me, 2), :, pl.ds(pl.multiple_of(lax.rem(me, 2) * DK, DK), DK), :] = ent[me]
    pass_strip(1)
    pass_strip(2)


    def outer_step(i, carry):
        p = lax.rem(lax.div(me, 2) + PAIRS - i, PAIRS)
        for hh in range(2):
            h = 2 * p + hh

            @pl.when(h != me)
            def _():
                remote(enm.at[h], esm.at[h], sd.at[h], rd.at[h], h).wait_recv()
                entry_in(0, h, se, re).wait_recv()
                entry_in(1, h, seb, reb).wait_recv()

        cols = pl.ds(pl.multiple_of(p * C, C), C)
        lhs = lhs_of(cols)
        carried = jnp.dot(lhs, jnp.concatenate([est[p, 0], est[p, 1]], axis=1), preferred_element_type=F32)
        nf_row = jnp.where(low_row, esm[2 * p, 0:1], esm[2 * p + 1, 0:1])
        nb_row = jnp.where(low_row, esm[2 * p, 1:2], esm[2 * p + 1, 1:2])
        lhs32 = lhs.astype(F32)
        zf_all = jnp.sum(lhs32 * nf_row, axis=1, keepdims=True)
        zb_all = jnp.sum(lhs32 * nb_row, axis=1, keepdims=True)
        for hh in range(2):
            h = 2 * p + hh
            part = slice(hh * C, (hh + 1) * C)
            grow_f = jnp.exp(fcol[h])
            grow_b = jnp.exp(bcol[h])
            zf = zfb[h, 0:C] + grow_f * zf_all[part]
            zb = zfb[h, C:2 * C] + grow_b * zb_all[part]
            nf = nfb[h, 0:C] + grow_f * carried[part, 0:DV]
            nb = nfb[h, C:2 * C] + grow_b * carried[part, DV:2 * DV]
            total = nf / jnp.maximum(jnp.abs(zf), 1.0) + nb / jnp.maximum(jnp.abs(zb), 1.0)
            mean = jnp.mean(total * total, axis=1, keepdims=True)
            mixed = (total * lax.rsqrt(mean + EPS) * rx1[h, 1:2]).astype(BF16)
            vcols = pl.ds(pl.multiple_of(h * DV, DV), DV)
            gated[:, vcols] = (mixed.astype(F32) * sg[:, vcols]).astype(BF16)
        return carry

    lax.fori_loop(0, PAIRS, outer_step, 0)

    def project(shard):
        cols = pl.ds(pl.multiple_of(shard * 256, 256), 256)
        proj[:, cols] = jnp.dot(gated[...], wbuf[shard], preferred_element_type=F32)

    for n in range(1, 8):
        pl.semaphore_signal(meet, inc=1, device_id=(me, lax.rem(dp + n, 8)), device_id_type=MESH)
    each_peer(lambda p: pl.semaphore_signal(meet, inc=1, device_id=(p, dp), device_id_type=MESH))
    project(dp)
    for n in range(2, 4):
        to_right(left, n, n).wait_recv()
        to_left(right, n - 2, n).wait_recv()
    strips(0).wait_recv()
    to_partner(wbuf.at[left], 1).start()
    project(left)
    strips(1).wait_recv()
    to_partner(wbuf.at[right], 2).start()
    project(right)
    strips(2).wait_recv()
    edge = pl.ds(0, BASE)
    to_partner(wbuf.at[across, edge, :], 3).start()
    far = 1 - 2 * core
    to_partner(wbuf.at[partner], 0).wait_recv()
    project(partner)
    for n in range(2):
        to_right(across, n, 4 + n).wait_recv()
        to_partner(piece(across, n), 4 + n).start()
        to_left(across, n + 2, 4 + n).wait_recv()
        to_partner(piece(across, n + 2), 6 + n).start()
    to_partner(wbuf.at[left + far], 1).wait_recv()
    project(left + far)
    to_partner(wbuf.at[right + far], 2).wait_recv()
    project(right + far)
    project(across)
    to_partner(wbuf.at[across + far, edge, :], 3).wait_recv()
    for n in range(2):
        to_partner(piece(across + far, n), 4 + n).wait_recv()
        to_partner(piece(across + far, n + 2), 6 + n).wait_recv()
    project(across + far)

    local[14].wait()
    pr = proj[...]
    scale = lax.rsqrt(jnp.mean(pr * pr, axis=1, keepdims=True) + EPS)
    stream = (res_ref[...].astype(F32) + cng_ref[...] * pr * scale).astype(BF16).astype(F32)
    proj[...] = stream
    scale = lax.rsqrt(jnp.mean(stream * stream, axis=1, keepdims=True) + EPS)
    gated[...] = (eng_ref[...] * stream * scale).astype(BF16)

    def route_of(j, i):
        t = lax.rem(i * STRIDE, PER)
        dc = lax.rem(t, 2)
        dx = lax.rem(lax.div(t, 2), 4)
        dy = lax.div(t, 8)
        dz = lax.rem(j + 8 - dx - dy, 4)
        return j * PER + t, dz, dy, dx, dc

    def onward(j, i):
        place, dz, dy, dx, dc = route_of(j, i)
        sp_to = lax.rem(z + dz, 4) * 4 + lax.rem(y + dy, 4)
        dp_to = lax.rem(x + dx, 4) * 2 + lax.rem(core + dc, 2)
        return place, (sp_to, dp_to)

    def homeward(j, i):
        place, dz, dy, dx, dc = route_of(j, i)
        sp_to = lax.rem(z + 4 - dz, 4) * 4 + lax.rem(y + 4 - dy, 4)
        dp_to = lax.rem(x + 4 - dx, 4) * 2 + lax.rem(core + dc, 2)
        return place, (sp_to, dp_to)

    def send_chunk(j, way, src, dst, ssem, rsem):
        def step(i, carry):
            place, where = way(j, i)

            @pl.when(place != 0)
            def _():
                copy_to(src.at[place], dst.at[place], ssem.at[j], rsem.at[j], where).start()

            return carry

        lax.fori_loop(0, PER, step, 0)

    def whole(j, src, dst, ssem, rsem):
        span = pl.ds(1, PER - 1) if j == 0 else pl.ds(j * PER, PER)
        return copy_to(src.at[span], dst.at[span], ssem.at[j], rsem.at[j], (me, partner))

    for j in range(CHUNKS):
        rows_out = lax.dot_general(
            tab_send[:, j * C:(j + 1) * C], gated[...], TN, preferred_element_type=F32)
        outgoing[j * PER:(j + 1) * PER] = rows_out.astype(BF16).reshape(PER, CAP, D)
        if j == 0:
            pl.semaphore_wait(meet, H - 1 + 7)
        send_chunk(j, onward, outgoing, arrived, ds, dr)
        if j == 0:
            arrived[0] = outgoing[0]

    for c in local[15:]:
        c.wait()

    def expert_chunk(j):
        rows_in = arrived[pl.ds(j * PER, PER)].reshape(PER * CAP, D)
        a = jnp.dot(rows_in, gate_w[...], preferred_element_type=F32)
        b = jnp.dot(rows_in, up_w[...], preferred_element_type=F32)
        hidden = (a / (1.0 + jnp.exp(-a)) * b).astype(BF16)
        made = jnp.dot(hidden, down_w[...], preferred_element_type=F32).astype(BF16)
        produced[pl.ds(j * PER, PER)] = made.reshape(PER, CAP, D)

    def expert_step(j, carry):
        for n in range(CHUNKS):
            @pl.when(j == n)
            def _():
                whole(n, outgoing, arrived, ds, dr).wait_recv()

        @pl.when(j >= 1)
        def _():
            send_chunk(j - 1, homeward, produced, returned, bs, br)

        expert_chunk(j)
        return carry

    lax.fori_loop(0, CHUNKS, expert_step, 0)
    for j in range(CHUNKS - 1, CHUNKS):
        send_chunk(j, homeward, produced, returned, bs, br)
    returned[0] = produced[0]

    for j in range(CHUNKS):
        whole(j, produced, returned, bs, br).wait_recv()
        rows_back = returned[j * PER:(j + 1) * PER].reshape(PER * CAP, D)
        parts = jnp.dot(tab_back[:, j * C:(j + 1) * C], rows_back, preferred_element_type=F32)
        proj[...] += parts[0:C] + parts[C:2 * C]
    out_ref[...] = proj[...].astype(BF16)

    each_peer(lambda p: remote(msg.at[p], rx1.at[me], sa.at[p], ra.at[me], p).wait_send())
    each_peer(lambda p: remote(lsm.at[p], rxm.at[me], sc.at[p], rc.at[me], p).wait_send())
    each_peer(lambda p: state_out(0, p, sb, rb).wait_send())
    each_peer(lambda p: state_out(1, p, sbb, rbb).wait_send())
    each_peer(lambda p: remote(enm.at[p], esm.at[me], sd.at[p], rd.at[me], p).wait_send())
    each_peer(lambda p: entry_out(0, p, se, re).wait_send())
    each_peer(lambda p: entry_out(1, p, seb, reb).wait_send())
    for n in range(6):
        to_right(dp, 0, n).wait_send()
        to_left(dp, 0, n).wait_send()
    for n in range(3):
        to_partner(wbuf.at[dp], n).wait_send()
    to_partner(wbuf.at[dp, edge, :], 3).wait_send()
    for n in range(4, 8):
        to_partner(piece(dp, 0), n).wait_send()
    for n in range(3):
        strip_out(n).wait_send()
        strips(n).wait_send()
    for j in range(CHUNKS):
        whole(j, outgoing, arrived, ds, dr).wait_send()
        whole(j, produced, returned, bs, br).wait_send()


def on_device(
    residual_input, queries, keys, values, gate_logits, retention_offset, log_forget_extra,
    lane_amplifier, output_gate_logits, output_projection, cell_norm_gain, expert_norm_gain,
    expert_index, group_mixing_weight, within_group_weight, gate_weight, up_weight, down_weight,
):
    vm = pl.BlockSpec(memory_space=pltpu.VMEM)
    hbm = pl.BlockSpec(memory_space=pl.ANY)
    dma = pltpu.SemaphoreType.DMA
    small = pltpu.VMEM((H, 8, C), F32)
    state = pltpu.VMEM((H, 2, DK, DV), BF16)
    slots = pltpu.VMEM((DEVICES, CAP, D), BF16)
    out = pl.pallas_call(
        layer_kernel,
        out_shape=jax.ShapeDtypeStruct((C, D), BF16),
        in_specs=[hbm] * 18,
        out_specs=vm,
        scratch_shapes=[
            pltpu.VMEM((4 * H, C), BF16),
            pltpu.VMEM((H, C), F32),
            pltpu.VMEM((1, C), F32),
            pltpu.VMEM((1, 2), F32),
            pltpu.VMEM((2, C), jnp.int32),
            pltpu.VMEM((4, C), F32),
            pltpu.VMEM((2, C), F32),
            pltpu.VMEM((1, D), F32),
            pltpu.VMEM((1, D), F32),
            pltpu.VMEM((C, H * DK), BF16),
            pltpu.VMEM((C, H * DK), BF16),
            pltpu.VMEM((C, H * DV), BF16),
            pltpu.VMEM((C, H * DV), BF16),
            pltpu.VMEM((C, D), BF16),
            pltpu.VMEM((8, D, 256), BF16),
            pltpu.VMEM((D, FF), BF16),
            pltpu.VMEM((D, FF), BF16),
            pltpu.VMEM((FF, D), BF16),
            small, small, state, small, state, small, state, small,
            pltpu.VMEM((PAIRS, 2, 2 * DK, DV), BF16),
            small,
            pltpu.VMEM((4 * H, C), F32),
            pltpu.VMEM((H, C, C), F32),
            pltpu.VMEM((H, C, C), F32),
            pltpu.VMEM((3, H, C), F32),
            pltpu.VMEM((PAIRS, 2, C, C), F32),
            pltpu.VMEM((H, 2 * C, DV), F32),
            pltpu.VMEM((H, 2 * C, C), F32),
            pltpu.VMEM((C, H * DV), F32),
            pltpu.VMEM((C, H * DV), BF16),
            pltpu.VMEM((C, D), F32),
            pltpu.VMEM((C, DEVICES * CAP), BF16),
            pltpu.VMEM((2 * C, DEVICES * CAP), BF16),
            slots, slots, slots, slots,
            dma((18,)),
        ] + [dma((H,))] * 14 + [dma((6,))] * 4 + [dma((8,))] * 2 + [dma((3,))] * 4 + [dma((CHUNKS,))] * 4 + [pltpu.SemaphoreType.REGULAR],
        compiler_params=pltpu.CompilerParams(
            collective_id=0, has_side_effects=True, vmem_limit_bytes=67_043_328),
        name="layer",
    )(
        queries[0], keys[0], values[0], output_gate_logits[0], residual_input[0], output_projection,
        gate_weight[0], up_weight[0], down_weight[0],
        gate_logits[0].T, log_forget_extra.reshape(H, C), lane_amplifier.reshape(1, C), retention_offset,
        expert_index[0].T, group_mixing_weight[0].T, within_group_weight[0].T,
        cell_norm_gain.reshape(1, D), expert_norm_gain.reshape(1, D),
    )
    return out.reshape(1, C, D)


def solution(mesh):
    by_place = P("dp", "sp", None)
    by_expert = P(("sp", "dp"), None, None)
    in_specs = (
        by_place, by_place, by_place, by_place, by_place, P("sp", None), by_place, P("sp"), by_place,
        P(None, "dp"), P(), P(), by_place, by_place, by_place, by_expert, by_expert, by_expert,
    )
    return jax.shard_map(on_device, mesh=mesh, in_specs=in_specs, out_specs=by_place, check_vma=False)
```

```python
import jax
import jax.numpy as jnp
from jax import lax
from jax.experimental import pallas as pl
from jax.experimental.pallas import tpu as pltpu
from jax.sharding import PartitionSpec as P

EPS = 1e-06
HIGH = lax.Precision.HIGHEST
F32 = jnp.float32
BF16 = jnp.bfloat16
H = 16
DK = 64
DV = 128
C = 128
D = 2048
FF = 1024
CAP = 4
DEVICES = 128
CHUNKS = 4
PER = DEVICES // CHUNKS
PAIRS = H // 2
STRIDE = 7
PIECE = 32
BASE = H * PIECE
QUARTER = (D - BASE) // 4
NT = (((1,), (1,)), ((), ()))
TN = (((0,), (0,)), ((), ()))
MESH = pl.DeviceIdType.MESH


def log_sigmoid(x):
    return jnp.minimum(x, 0.0) - jnp.log1p(jnp.exp(-jnp.abs(x)))


def layer_kernel(
    q_hbm, k_hbm, v_hbm, ogl_hbm, res_hbm, wo_hbm, gate_hbm, up_hbm, down_hbm,
    g_hbm, ext_hbm, lam_hbm, ro_hbm, ids_hbm, group_hbm, within_hbm, cng_hbm, eng_hbm,
    out_ref,
    g_ref, ext_ref, lam_ref, ro_ref, ids_ref, group_ref, within_ref, cng_ref, eng_ref,
    q_ref, k_ref, v_ref, ogl_ref, res_ref, wbuf, gate_w, up_w, down_w,
    msg, rx1, lst, lsm, rxs, rxm, ent, enm, est, esm,
    gates, fcol, bcol, rows, wpair, nfb, zfb, sg,
    gated, proj, tab_send, tab_back, outgoing, arrived, produced, returned,
    loc, sa, ra, sb, rb, sbb, rbb, sc, rc, sd, rd, se, re, seb, reb,
    wsr, wsl, wrl, wrr, wps, wpr, pxs, pxr, pys, pyr, ds, dr, bs, br, meet,
):
    me = lax.axis_index("sp")
    dp = lax.axis_index("dp")
    z, y = lax.div(me, 4), lax.rem(me, 4)
    x, core = lax.div(dp, 2), lax.rem(dp, 2)
    flat = me * 8 + dp

    def peer_of(d):
        return lax.rem(me + d, H)

    def copy_to(src, dst, ssem, rsem, where):
        return pltpu.make_async_remote_copy(
            src_ref=src, dst_ref=dst, send_sem=ssem, recv_sem=rsem,
            device_id=where, device_id_type=MESH,
        )

    def remote(src, dst, ssem, rsem, peer):
        return copy_to(src, dst, ssem, rsem, (peer, dp))

    def fifteen(src, dst, ssem, rsem):
        most = pl.ds(0, H - 1)
        return remote(src.at[most], dst.at[most], ssem.at[0], rsem.at[0], peer_of(1))

    def each_peer(body):
        def step(d, carry):
            body(peer_of(d))
            return carry

        lax.fori_loop(1, H, step, 0)

    barrier = pltpu.get_barrier_semaphore()

    def greet(where):
        pl.semaphore_signal(barrier, inc=1, device_id=where, device_id_type=MESH)

    each_peer(lambda p: greet((p, dp)))
    for n in range(1, 8):
        greet((me, lax.rem(dp + n, 8)))

    local = [
        pltpu.make_async_copy(src, dst, loc.at[i])
        for i, (src, dst) in enumerate((
            (ext_hbm, ext_ref), (lam_hbm, lam_ref), (ro_hbm, ro_ref), (g_hbm, g_ref),
            (wo_hbm, wbuf.at[dp]), (k_hbm, k_ref), (v_hbm, v_ref), (q_hbm, q_ref), (ogl_hbm, ogl_ref),
            (ids_hbm, ids_ref), (group_hbm, group_ref), (within_hbm, within_ref),
            (cng_hbm, cng_ref), (eng_hbm, eng_ref),
            (res_hbm, res_ref), (gate_hbm, gate_w), (up_hbm, up_w), (down_hbm, down_w),
        ))
    ]
    for c in local[:14]:
        c.start()

    lane = lax.broadcasted_iota(jnp.int32, (C, C), 1)
    row_id = lax.broadcasted_iota(jnp.int32, (C, C), 0)
    low_half = lane < DK
    low_row = low_half[0:1]
    earlier = lane <= row_id
    diagonal = lane == row_id

    for c in local[:4]:
        c.wait()
    msg[:, 0, :] = ext_ref[...]
    msg[:, 1, :] = jnp.broadcast_to(lam_ref[...], (H, C))
    msg[:, 2, :] = jnp.broadcast_to(ro_ref[:, 0:1], (H, C))
    msg[:, 3, :] = jnp.broadcast_to(ro_ref[:, 1:2], (H, C))
    for i in range(4, 8):
        msg[:, i, :] = jnp.zeros((H, C), F32)
    gates[...] = g_ref[...].astype(F32)
    pl.semaphore_wait(barrier, H - 1 + 7)

    each_peer(lambda p: remote(msg.at[p], rx1.at[me], sa.at[0], ra.at[0], p).start())
    rx1[me] = msg[me]

    right = lax.rem(x + 1, 4) * 2 + core
    left = lax.rem(x + 3, 4) * 2 + core
    across = lax.rem(x + 2, 4) * 2 + core
    partner = x * 2 + 1 - core

    def piece(shard, i):
        return wbuf.at[shard, pl.ds(BASE + i * QUARTER, QUARTER), :]

    def strip(shard, owner):
        return wbuf.at[shard, pl.ds(pl.multiple_of(owner * PIECE, PIECE), PIECE), :]

    others = ((right, left), (left, right), (across, across))

    def strip_out(n):
        ref = strip(dp, me)
        return copy_to(ref, ref, pxs.at[n], pxr.at[n], (me, others[n][0]))

    def strip_on(n, peer):
        ref = strip(others[n][1], me)
        return copy_to(ref, ref, pys.at[n], pyr.at[n], (peer, dp))

    def strips(n):
        ref = wbuf.at[others[n][1], pl.ds(0, BASE - PIECE), :]
        return copy_to(ref, ref, pys.at[n], pyr.at[n], (me, partner))

    def pass_strip(n):
        strip_out(n).wait_recv()
        each_peer(lambda p: strip_on(n, p).start())

    def to_right(shard, i, n):
        return copy_to(piece(shard, i), piece(shard, i), wsr.at[n], wrl.at[n], (me, right))

    def to_left(shard, i, n):
        return copy_to(piece(shard, i), piece(shard, i), wsl.at[n], wrr.at[n], (me, left))

    def to_partner(ref, n):
        return copy_to(ref, ref, wps.at[n], wpr.at[n], (me, partner))

    local[4].wait()
    for n in range(3):
        strip_out(n).start()
    for n in range(4):
        to_right(dp, n, n).start()
        to_left(dp, (n + 2) % 4, n).start()
    to_partner(wbuf.at[dp], 0).start()
    for c in local[5:14]:
        c.wait()
    for c in local[14:]:
        c.start()

    def gate_step(p, carry):
        cols = pl.ds(pl.multiple_of(p * 256, 256), 256)
        sg[:, cols] = 1.0 / (1.0 + jnp.exp(-ogl_ref[:, cols].astype(F32)))
        return carry

    lax.fori_loop(0, PAIRS, gate_step, 0)

    pass_strip(0)
    table_in = jnp.concatenate(
        [ids_ref[...].astype(F32), group_ref[...], within_ref[...], jnp.zeros((C - 8, C), F32)], axis=0).T
    wide = lax.broadcasted_iota(jnp.int32, (C, DEVICES * CAP), 1)
    hits, targets, routes = [], [], []
    for n in range(2):
        expert = table_in[:, n:n + 1].astype(jnp.int32)
        dz = jnp.bitwise_and(jnp.right_shift(expert, 5) - z + 4, 3)
        dy = jnp.bitwise_and(jnp.right_shift(expert, 3) - y + 8, 3)
        dx = jnp.bitwise_and(jnp.right_shift(expert, 1) - x + 4, 3)
        dc = jnp.bitwise_and(expert - core + 2, 1)
        place = jnp.bitwise_and(dz + dy + dx, 3) * PER + dy * 8 + dx * 2 + dc
        group = jnp.right_shift(expert, 5)
        share = jnp.zeros((C, 1), F32)
        for i in range(4):
            share = share + jnp.where(group == i, table_in[:, 2 + i:3 + i], 0.0)
        routes.append(share * table_in[:, 6 + n:7 + n])
        targets.append(place * CAP)
        hits.append((lane == place).astype(F32))
    before = jnp.dot((lane < row_id).astype(BF16), (hits[0] + hits[1]).astype(BF16), preferred_element_type=F32)
    sent = jnp.zeros((C, DEVICES * CAP), F32)
    back = jnp.zeros((C, DEVICES * CAP), F32)
    for n in range(2):
        nth = jnp.sum(before * hits[n], axis=1, keepdims=True).astype(jnp.int32)
        chosen = wide == targets[n] + nth
        sent = sent + jnp.where(chosen, 1.0, 0.0)
        back = back + jnp.where(chosen, routes[n], 0.0)
    tab_send[...] = sent.astype(BF16)
    back_hi = back.astype(BF16)
    tab_back[0:C] = back_hi
    tab_back[C:2 * C] = (back - back_hi.astype(F32)).astype(BF16)

    fifteen(msg, rx1, sa, ra).wait_recv()

    spread = rx1[:, 0, :]
    in_f = gates[pl.ds(0, H, stride=4), :]
    in_b = gates[pl.ds(2, H, stride=4), :]
    fade_f = log_sigmoid(gates[pl.ds(1, H, stride=4), :] + rx1[:, 2, :]) + spread
    fade_b = log_sigmoid(gates[pl.ds(3, H, stride=4), :] + rx1[:, 3, :]) + spread
    upto = (row_id <= lane).astype(F32)
    since = (row_id >= lane).astype(F32)
    cum_f = jnp.dot(fade_f, upto, precision=HIGH, preferred_element_type=F32)
    cum_b = jnp.dot(fade_b, since, precision=HIGH, preferred_element_type=F32)
    end_f = jnp.broadcast_to(cum_f[:, C - 1:C], (H, C))
    end_b = jnp.broadcast_to(cum_b[:, 0:1], (H, C))
    w_f = jnp.exp(end_f - cum_f + in_f)
    w_b = jnp.exp(end_b - cum_b + in_b)
    rows[0] = cum_f - in_f
    rows[1] = cum_b - in_b
    rows[2] = jnp.exp(in_b)
    turned = jnp.concatenate([cum_f, cum_b, w_f, w_b, jnp.zeros((C - 4 * H, C), F32)], axis=0).T
    wf_hi = w_f.astype(BF16)
    wb_hi = w_b.astype(BF16)
    wf_lo = (w_f - wf_hi.astype(F32)).astype(BF16)
    wb_lo = (w_b - wb_hi.astype(F32)).astype(BF16)
    stacked = jnp.concatenate([wf_hi, wf_lo, wb_hi, wb_lo], axis=0)
    norm = jnp.dot(stacked, k_ref[...], preferred_element_type=F32)
    norm_f = norm[0:16] + norm[16:32]
    norm_b = norm[32:48] + norm[48:64]
    for p in range(PAIRS):
        h0, h1 = 2 * p, 2 * p + 1
        wpair[p, 0] = jnp.where(low_half, turned[:, 32 + h0:33 + h0], turned[:, 32 + h1:33 + h1])
        wpair[p, 1] = jnp.where(low_half, turned[:, 48 + h0:49 + h0], turned[:, 48 + h1:49 + h1])
        for h, keep in ((h0, low_row), (h1, ~low_row)):
            nf = norm_f[h:h + 1, p * C:(p + 1) * C]
            nb = norm_b[h:h + 1, p * C:(p + 1) * C]
            nf = jnp.where(keep, nf, pltpu.roll(nf, DK, 1))
            nb = jnp.where(keep, nb, pltpu.roll(nb, DK, 1))
            lsm[h] = jnp.concatenate(
                [nf, nb, end_f[h:h + 1], end_b[h:h + 1], jnp.zeros((4, C), F32)], axis=0)

    each_peer(lambda p: remote(lsm.at[p], rxm.at[me], sc.at[0], rc.at[0], p).start())
    rxm[me] = lsm[me]
    first = lax.div(me, 2) + 1

    def state_out(way, h, ssem, rsem):
        return remote(lst.at[h, way], rxs.at[me, way], ssem.at[0], rsem.at[0], h)

    def states_in(way, ssem, rsem):
        most = pl.ds(0, H - 1)
        return remote(lst.at[most, way], rxs.at[most, way], ssem.at[0], rsem.at[0], peer_of(1))

    def post_pair(i):
        p = lax.rem(first + i, PAIRS)
        for hh in range(2):
            h = 2 * p + hh

            @pl.when(h != me)
            def _():
                state_out(0, h, sb, rb).start()

    def state_step(i, carry):
        p = lax.rem(first + i, PAIRS)
        k32 = k_ref[:, pl.ds(pl.multiple_of(p * C, C), C)].astype(F32)
        both = jnp.concatenate([k32 * wpair[p, 0], k32 * wpair[p, 1]], axis=1).astype(BF16)
        vp = v_ref[:, pl.ds(pl.multiple_of(p * 256, 256), 256)]
        state = lax.dot_general(both, vp, TN, preferred_element_type=F32).astype(BF16)
        lst[2 * p, 0] = state[0:64, 0:128]
        lst[2 * p + 1, 0] = state[64:128, 128:256]
        lst[2 * p, 1] = state[128:192, 0:128]
        lst[2 * p + 1, 1] = state[192:256, 128:256]

        @pl.when(i > 0)
        def _():
            post_pair(i - 1)

        return carry

    lax.fori_loop(0, PAIRS, state_step, 0)
    post_pair(PAIRS - 1)
    each_peer(lambda p: state_out(1, p, sbb, rbb).start())
    rxs[me] = lst[me]

    def relay(n):
        to_right(left, n, n).wait_recv()
        to_right(left, n, 4 + n).start()
        to_left(right, n + 2, n).wait_recv()
        to_left(right, n + 2, 4 + n).start()


    for h in range(H):
        fcol[h] = jnp.broadcast_to(turned[:, h:h + 1], (C, C))
        bcol[h] = jnp.broadcast_to(turned[:, 16 + h:17 + h], (C, C))

    relay(0)

    def lhs_of(cols):
        qp = q_ref[:, cols] * jnp.asarray(DK ** -0.5, BF16)
        none = jnp.zeros_like(qp)
        return jnp.concatenate([jnp.where(low_half, qp, none), jnp.where(low_half, none, qp)], axis=0)

    def inner_step(p, carry):
        cols = pl.ds(pl.multiple_of(p * C, C), C)
        score2 = lax.dot_general(lhs_of(cols), k_ref[:, cols], NT, preferred_element_type=F32)
        for hh in range(2):
            h = 2 * p + hh
            score = score2[hh * C:(hh + 1) * C]
            ahead = fcol[h] - rows[0, pl.ds(h, 1), :]
            behind = bcol[h] - rows[1, pl.ds(h, 1), :]
            weighted = score * jnp.exp(jnp.where(earlier, ahead, behind))
            pf = jnp.where(earlier, weighted, 0.0)
            pb = jnp.where(earlier, jnp.where(diagonal, score * rows[2, pl.ds(h, 1), :], 0.0), weighted)
            both = jnp.concatenate([pf, pb], axis=0)
            zfb[h] = jnp.broadcast_to(jnp.sum(both, axis=1, keepdims=True), (2 * C, C))
            vcols = pl.ds(pl.multiple_of(h * DV, DV), DV)
            nfb[h] = jnp.dot(both.astype(BF16), v_ref[:, vcols], preferred_element_type=F32)
        return carry

    lax.fori_loop(0, PAIRS, inner_step, 0)

    relay(1)
    fifteen(lsm, rxm, sc, rc).wait_recv()
    enm[...] = jnp.zeros_like(enm)

    def slot(way, h):
        return est.at[lax.div(h, 2), way, pl.ds(pl.multiple_of(lax.rem(h, 2) * DK, DK), DK), :]

    def entry_out(way, p, ssem, rsem):
        return remote(ent.at[p, way], slot(way, me), ssem.at[0], rsem.at[me], p)

    def entry_in(way, p, ssem, rsem):
        return remote(ent.at[p, way], slot(way, p), ssem.at[0], rsem.at[p], p)

    def run(way, ssem, rsem, ssem_out, rsem_out):
        states_in(way, ssem, rsem).wait_recv()

        def carry_step(i, state):
            m, n = state
            c = i if way == 0 else H - 1 - i
            ent[c, way] = m.astype(BF16)
            enm[c, way:way + 1] = n
            keep = jnp.exp(rxm[c, 2 + way:3 + way])
            return m * keep + rxs[c, way].astype(F32), n * keep + rxm[c, way:way + 1]

        lax.fori_loop(0, H, carry_step, (jnp.zeros((DK, DV), F32), jnp.zeros((1, C), F32)))
        each_peer(lambda p: entry_out(way, p, ssem_out, rsem_out).start())

    run(0, sb, rb, se, re)
    run(1, sbb, rbb, seb, reb)
    each_peer(lambda p: remote(enm.at[p], esm.at[me], sd.at[0], rd.at[me], p).start())
    esm[me] = enm[me]
    est[lax.div(me, 2), :, pl.ds(pl.multiple_of(lax.rem(me, 2) * DK, DK), DK), :] = ent[me]
    pass_strip(1)
    pass_strip(2)


    def outer_step(i, carry):
        p = lax.rem(lax.div(me, 2) + PAIRS - i, PAIRS)
        for hh in range(2):
            h = 2 * p + hh

            @pl.when(h != me)
            def _():
                remote(enm.at[h], esm.at[h], sd.at[0], rd.at[h], h).wait_recv()
                entry_in(0, h, se, re).wait_recv()
                entry_in(1, h, seb, reb).wait_recv()

        cols = pl.ds(pl.multiple_of(p * C, C), C)
        lhs = lhs_of(cols)
        carried = jnp.dot(lhs, jnp.concatenate([est[p, 0], est[p, 1]], axis=1), preferred_element_type=F32)
        nf_row = jnp.where(low_row, esm[2 * p, 0:1], esm[2 * p + 1, 0:1])
        nb_row = jnp.where(low_row, esm[2 * p, 1:2], esm[2 * p + 1, 1:2])
        lhs32 = lhs.astype(F32)
        zf_all = jnp.sum(lhs32 * nf_row, axis=1, keepdims=True)
        zb_all = jnp.sum(lhs32 * nb_row, axis=1, keepdims=True)
        for hh in range(2):
            h = 2 * p + hh
            part = slice(hh * C, (hh + 1) * C)
            grow_f = jnp.exp(fcol[h])
            grow_b = jnp.exp(bcol[h])
            zf = zfb[h, 0:C] + grow_f * zf_all[part]
            zb = zfb[h, C:2 * C] + grow_b * zb_all[part]
            nf = nfb[h, 0:C] + grow_f * carried[part, 0:DV]
            nb = nfb[h, C:2 * C] + grow_b * carried[part, DV:2 * DV]
            total = nf / jnp.maximum(jnp.abs(zf), 1.0) + nb / jnp.maximum(jnp.abs(zb), 1.0)
            mean = jnp.mean(total * total, axis=1, keepdims=True)
            mixed = (total * lax.rsqrt(mean + EPS) * rx1[h, 1:2]).astype(BF16)
            vcols = pl.ds(pl.multiple_of(h * DV, DV), DV)
            gated[:, vcols] = (mixed.astype(F32) * sg[:, vcols]).astype(BF16)
        return carry

    lax.fori_loop(0, PAIRS, outer_step, 0)

    def project(shard):
        cols = pl.ds(pl.multiple_of(shard * 256, 256), 256)
        proj[:, cols] = jnp.dot(gated[...], wbuf[shard], preferred_element_type=F32)

    for n in range(1, 8):
        pl.semaphore_signal(meet, inc=1, device_id=(me, lax.rem(dp + n, 8)), device_id_type=MESH)
    each_peer(lambda p: pl.semaphore_signal(meet, inc=1, device_id=(p, dp), device_id_type=MESH))
    project(dp)
    for n in range(2, 4):
        to_right(left, n, n).wait_recv()
        to_left(right, n - 2, n).wait_recv()
    strips(0).wait_recv()
    to_partner(wbuf.at[left], 1).start()
    project(left)
    strips(1).wait_recv()
    to_partner(wbuf.at[right], 2).start()
    project(right)
    strips(2).wait_recv()
    edge = pl.ds(0, BASE)
    to_partner(wbuf.at[across, edge, :], 3).start()
    far = 1 - 2 * core
    to_partner(wbuf.at[partner], 0).wait_recv()
    project(partner)
    for n in range(2):
        to_right(across, n, 4 + n).wait_recv()
        to_partner(piece(across, n), 4 + n).start()
        to_left(across, n + 2, 4 + n).wait_recv()
        to_partner(piece(across, n + 2), 6 + n).start()
    to_partner(wbuf.at[left + far], 1).wait_recv()
    project(left + far)
    to_partner(wbuf.at[right + far], 2).wait_recv()
    project(right + far)
    project(across)
    to_partner(wbuf.at[across + far, edge, :], 3).wait_recv()
    for n in range(2):
        to_partner(piece(across + far, n), 4 + n).wait_recv()
        to_partner(piece(across + far, n + 2), 6 + n).wait_recv()
    project(across + far)

    local[14].wait()
    pr = proj[...]
    scale = lax.rsqrt(jnp.mean(pr * pr, axis=1, keepdims=True) + EPS)
    stream = (res_ref[...].astype(F32) + cng_ref[...] * pr * scale).astype(BF16).astype(F32)
    proj[...] = stream
    scale = lax.rsqrt(jnp.mean(stream * stream, axis=1, keepdims=True) + EPS)
    gated[...] = (eng_ref[...] * stream * scale).astype(BF16)

    def route_of(j, i):
        t = lax.rem(i * STRIDE, PER)
        dc = lax.rem(t, 2)
        dx = lax.rem(lax.div(t, 2), 4)
        dy = lax.div(t, 8)
        dz = lax.rem(j + 8 - dx - dy, 4)
        return j * PER + t, dz, dy, dx, dc

    def onward(j, i):
        place, dz, dy, dx, dc = route_of(j, i)
        sp_to = lax.rem(z + dz, 4) * 4 + lax.rem(y + dy, 4)
        dp_to = lax.rem(x + dx, 4) * 2 + lax.rem(core + dc, 2)
        return place, (sp_to, dp_to)

    def homeward(j, i):
        place, dz, dy, dx, dc = route_of(j, i)
        sp_to = lax.rem(z + 4 - dz, 4) * 4 + lax.rem(y + 4 - dy, 4)
        dp_to = lax.rem(x + 4 - dx, 4) * 2 + lax.rem(core + dc, 2)
        return place, (sp_to, dp_to)

    def send_chunk(j, way, src, dst, ssem, rsem):
        def step(i, carry):
            place, where = way(j, i)

            @pl.when(place != 0)
            def _():
                copy_to(src.at[place], dst.at[place], ssem.at[j], rsem.at[j], where).start()

            return carry

        lax.fori_loop(0, PER, step, 0)

    def whole(j, src, dst, ssem, rsem):
        span = pl.ds(1, PER - 1) if j == 0 else pl.ds(j * PER, PER)
        return copy_to(src.at[span], dst.at[span], ssem.at[j], rsem.at[j], (me, partner))

    for j in range(CHUNKS):
        rows_out = lax.dot_general(
            tab_send[:, j * C:(j + 1) * C], gated[...], TN, preferred_element_type=F32)
        outgoing[j * PER:(j + 1) * PER] = rows_out.astype(BF16).reshape(PER, CAP, D)
        if j == 0:
            pl.semaphore_wait(meet, H - 1 + 7)
        send_chunk(j, onward, outgoing, arrived, ds, dr)
        if j == 0:
            arrived[0] = outgoing[0]

    for c in local[15:]:
        c.wait()
    fifteen(msg, rx1, sa, ra).wait_send()
    fifteen(lsm, rxm, sc, rc).wait_send()
    states_in(0, sb, rb).wait_send()
    states_in(1, sbb, rbb).wait_send()
    fifteen(enm, esm, sd, rc).wait_send()
    states_in(0, se, rb).wait_send()
    states_in(1, seb, rbb).wait_send()
    for n in range(6):
        to_right(dp, 0, n).wait_send()
        to_left(dp, 0, n).wait_send()
    for n in range(3):
        to_partner(wbuf.at[dp], n).wait_send()
    to_partner(wbuf.at[dp, edge, :], 3).wait_send()
    for n in range(4, 8):
        to_partner(piece(dp, 0), n).wait_send()
    for n in range(3):
        strip_out(n).wait_send()
        strips(n).wait_send()

    def expert_chunk(j):
        rows_in = arrived[pl.ds(j * PER, PER)].reshape(PER * CAP, D)
        a = jnp.dot(rows_in, gate_w[...], preferred_element_type=F32)
        b = jnp.dot(rows_in, up_w[...], preferred_element_type=F32)
        hidden = (a / (1.0 + jnp.exp(-a)) * b).astype(BF16)
        made = jnp.dot(hidden, down_w[...], preferred_element_type=F32).astype(BF16)
        produced[pl.ds(j * PER, PER)] = made.reshape(PER, CAP, D)

    def expert_step(j, carry):
        for n in range(CHUNKS):
            @pl.when(j == n)
            def _():
                whole(n, outgoing, arrived, ds, dr).wait_recv()

        @pl.when(j >= 1)
        def _():
            send_chunk(j - 1, homeward, produced, returned, bs, br)

        expert_chunk(j)
        return carry

    lax.fori_loop(0, CHUNKS, expert_step, 0)
    for j in range(CHUNKS - 1, CHUNKS):
        send_chunk(j, homeward, produced, returned, bs, br)
    returned[0] = produced[0]
    for j in range(CHUNKS):
        whole(j, outgoing, arrived, ds, dr).wait_send()

    for j in range(CHUNKS):
        whole(j, produced, returned, bs, br).wait_recv()
        rows_back = returned[j * PER:(j + 1) * PER].reshape(PER * CAP, D)
        parts = jnp.dot(tab_back[:, j * C:(j + 1) * C], rows_back, preferred_element_type=F32)
        proj[...] += parts[0:C] + parts[C:2 * C]
    out_ref[...] = proj[...].astype(BF16)

    for j in range(CHUNKS):
        whole(j, produced, returned, bs, br).wait_send()


def on_device(
    residual_input, queries, keys, values, gate_logits, retention_offset, log_forget_extra,
    lane_amplifier, output_gate_logits, output_projection, cell_norm_gain, expert_norm_gain,
    expert_index, group_mixing_weight, within_group_weight, gate_weight, up_weight, down_weight,
):
    vm = pl.BlockSpec(memory_space=pltpu.VMEM)
    hbm = pl.BlockSpec(memory_space=pl.ANY)
    dma = pltpu.SemaphoreType.DMA
    small = pltpu.VMEM((H, 8, C), F32)
    state = pltpu.VMEM((H, 2, DK, DV), BF16)
    slots = pltpu.VMEM((DEVICES, CAP, D), BF16)
    out = pl.pallas_call(
        layer_kernel,
        out_shape=jax.ShapeDtypeStruct((C, D), BF16),
        in_specs=[hbm] * 18,
        out_specs=vm,
        scratch_shapes=[
            pltpu.VMEM((4 * H, C), BF16),
            pltpu.VMEM((H, C), F32),
            pltpu.VMEM((1, C), F32),
            pltpu.VMEM((1, 2), F32),
            pltpu.VMEM((2, C), jnp.int32),
            pltpu.VMEM((4, C), F32),
            pltpu.VMEM((2, C), F32),
            pltpu.VMEM((1, D), F32),
            pltpu.VMEM((1, D), F32),
            pltpu.VMEM((C, H * DK), BF16),
            pltpu.VMEM((C, H * DK), BF16),
            pltpu.VMEM((C, H * DV), BF16),
            pltpu.VMEM((C, H * DV), BF16),
            pltpu.VMEM((C, D), BF16),
            pltpu.VMEM((8, D, 256), BF16),
            pltpu.VMEM((D, FF), BF16),
            pltpu.VMEM((D, FF), BF16),
            pltpu.VMEM((FF, D), BF16),
            small, small, state, small, state, small, state, small,
            pltpu.VMEM((PAIRS, 2, 2 * DK, DV), BF16),
            small,
            pltpu.VMEM((4 * H, C), F32),
            pltpu.VMEM((H, C, C), F32),
            pltpu.VMEM((H, C, C), F32),
            pltpu.VMEM((3, H, C), F32),
            pltpu.VMEM((PAIRS, 2, C, C), F32),
            pltpu.VMEM((H, 2 * C, DV), F32),
            pltpu.VMEM((H, 2 * C, C), F32),
            pltpu.VMEM((C, H * DV), F32),
            pltpu.VMEM((C, H * DV), BF16),
            pltpu.VMEM((C, D), F32),
            pltpu.VMEM((C, DEVICES * CAP), BF16),
            pltpu.VMEM((2 * C, DEVICES * CAP), BF16),
            slots, slots, slots, slots,
            dma((18,)),
        ] + [dma((1,))] * 9 + [dma((H,)), dma((1,)), dma((H,)), dma((1,)), dma((H,))] + [dma((6,))] * 4 + [dma((8,))] * 2 + [dma((3,))] * 4 + [dma((CHUNKS,))] * 4 + [pltpu.SemaphoreType.REGULAR],
        compiler_params=pltpu.CompilerParams(
            collective_id=0, has_side_effects=True, vmem_limit_bytes=67_043_328),
        name="layer",
    )(
        queries[0], keys[0], values[0], output_gate_logits[0], residual_input[0], output_projection,
        gate_weight[0], up_weight[0], down_weight[0],
        gate_logits[0].T, log_forget_extra.reshape(H, C), lane_amplifier.reshape(1, C), retention_offset,
        expert_index[0].T, group_mixing_weight[0].T, within_group_weight[0].T,
        cell_norm_gain.reshape(1, D), expert_norm_gain.reshape(1, D),
    )
    return out.reshape(1, C, D)


def solution(mesh):
    by_place = P("dp", "sp", None)
    by_expert = P(("sp", "dp"), None, None)
    in_specs = (
        by_place, by_place, by_place, by_place, by_place, P("sp", None), by_place, P("sp"), by_place,
        P(None, "dp"), P(), P(), by_place, by_place, by_place, by_expert, by_expert, by_expert,
    )
    return jax.shard_map(on_device, mesh=mesh, in_specs=in_specs, out_specs=by_place, check_vma=False)
```

```python
import jax
import jax.numpy as jnp
from jax import lax
from jax.experimental import pallas as pl
from jax.experimental.pallas import tpu as pltpu
from jax.sharding import PartitionSpec as P

EPS = 1e-06
HIGH = lax.Precision.HIGHEST
F32 = jnp.float32
BF16 = jnp.bfloat16
H = 16
DK = 64
DV = 128
C = 128
D = 2048
FF = 1024
CAP = 4
DEVICES = 128
CHUNKS = 4
PER = DEVICES // CHUNKS
PAIRS = H // 2
STRIDE = 7
PIECE = 32
BASE = H * PIECE
QUARTER = (D - BASE) // 4
NT = (((1,), (1,)), ((), ()))
TN = (((0,), (0,)), ((), ()))
MESH = pl.DeviceIdType.MESH


def log_sigmoid(x):
    return jnp.minimum(x, 0.0) - jnp.log1p(jnp.exp(-jnp.abs(x)))


def layer_kernel(
    q_hbm, k_hbm, v_hbm, ogl_hbm, res_hbm, wo_hbm, gate_hbm, up_hbm, down_hbm,
    g_hbm, ext_hbm, lam_hbm, ro_hbm, ids_hbm, group_hbm, within_hbm, cng_hbm, eng_hbm,
    out_ref,
    g_ref, ext_ref, lam_ref, ro_ref, ids_ref, group_ref, within_ref, cng_ref, eng_ref,
    q_ref, k_ref, v_ref, ogl_ref, res_ref, wbuf, gate_w, up_w, down_w,
    msg, rx1, lst, lsm, rxs, rxm, ent, enm, est, esm,
    gates, fcol, bcol, rows, wpair, nfb, zfb, sg,
    gated, proj, tab_send, tab_back, outgoing, arrived, produced, returned,
    loc, sa, ra, sb, rb, sbb, rbb, sc, rc, sd, rd, se, re, seb, reb,
    wsr, wsl, wrl, wrr, wps, wpr, pxs, pxr, pys, pyr, ds, dr, bs, br, meet,
):
    me = lax.axis_index("sp")
    dp = lax.axis_index("dp")
    z, y = lax.div(me, 4), lax.rem(me, 4)
    x, core = lax.div(dp, 2), lax.rem(dp, 2)
    flat = me * 8 + dp

    def peer_of(d):
        return lax.rem(me + d, H)

    def copy_to(src, dst, ssem, rsem, where):
        return pltpu.make_async_remote_copy(
            src_ref=src, dst_ref=dst, send_sem=ssem, recv_sem=rsem,
            device_id=where, device_id_type=MESH,
        )

    def remote(src, dst, ssem, rsem, peer):
        return copy_to(src, dst, ssem, rsem, (peer, dp))

    def fifteen(src, dst, ssem, rsem):
        most = pl.ds(0, H - 1)
        return remote(src.at[most], dst.at[most], ssem.at[0], rsem.at[0], peer_of(1))

    def each_peer(body):
        def step(d, carry):
            body(peer_of(d))
            return carry

        lax.fori_loop(1, H, step, 0, unroll=True)

    barrier = pltpu.get_barrier_semaphore()

    def greet(where):
        pl.semaphore_signal(barrier, inc=1, device_id=where, device_id_type=MESH)

    each_peer(lambda p: greet((p, dp)))
    for n in range(1, 8):
        greet((me, lax.rem(dp + n, 8)))

    local = [
        pltpu.make_async_copy(src, dst, loc.at[i])
        for i, (src, dst) in enumerate((
            (ext_hbm, ext_ref), (lam_hbm, lam_ref), (ro_hbm, ro_ref), (g_hbm, g_ref),
            (wo_hbm, wbuf.at[dp]), (k_hbm, k_ref), (v_hbm, v_ref), (q_hbm, q_ref), (ogl_hbm, ogl_ref),
            (ids_hbm, ids_ref), (group_hbm, group_ref), (within_hbm, within_ref),
            (cng_hbm, cng_ref), (eng_hbm, eng_ref),
            (res_hbm, res_ref), (gate_hbm, gate_w), (up_hbm, up_w), (down_hbm, down_w),
        ))
    ]
    for c in local[:14]:
        c.start()

    lane = lax.broadcasted_iota(jnp.int32, (C, C), 1)
    row_id = lax.broadcasted_iota(jnp.int32, (C, C), 0)
    low_half = lane < DK
    low_row = low_half[0:1]
    earlier = lane <= row_id
    diagonal = lane == row_id

    for c in local[:4]:
        c.wait()
    msg[:, 0, :] = ext_ref[...]
    msg[:, 1, :] = jnp.broadcast_to(lam_ref[...], (H, C))
    msg[:, 2, :] = jnp.broadcast_to(ro_ref[:, 0:1], (H, C))
    msg[:, 3, :] = jnp.broadcast_to(ro_ref[:, 1:2], (H, C))
    for i in range(4, 8):
        msg[:, i, :] = jnp.zeros((H, C), F32)
    gates[...] = g_ref[...].astype(F32)
    pl.semaphore_wait(barrier, H - 1 + 7)

    each_peer(lambda p: remote(msg.at[p], rx1.at[me], sa.at[0], ra.at[0], p).start())
    rx1[me] = msg[me]

    right = lax.rem(x + 1, 4) * 2 + core
    left = lax.rem(x + 3, 4) * 2 + core
    across = lax.rem(x + 2, 4) * 2 + core
    partner = x * 2 + 1 - core

    def piece(shard, i):
        return wbuf.at[shard, pl.ds(BASE + i * QUARTER, QUARTER), :]

    def strip(shard, owner):
        return wbuf.at[shard, pl.ds(pl.multiple_of(owner * PIECE, PIECE), PIECE), :]

    others = ((right, left), (left, right), (across, across))

    def strip_out(n):
        ref = strip(dp, me)
        return copy_to(ref, ref, pxs.at[n], pxr.at[n], (me, others[n][0]))

    def strip_on(n, peer):
        ref = strip(others[n][1], me)
        return copy_to(ref, ref, pys.at[n], pyr.at[n], (peer, dp))

    def strips(n):
        ref = wbuf.at[others[n][1], pl.ds(0, BASE - PIECE), :]
        return copy_to(ref, ref, pys.at[n], pyr.at[n], (me, partner))

    def pass_strip(n):
        strip_out(n).wait_recv()
        each_peer(lambda p: strip_on(n, p).start())

    def to_right(shard, i, n):
        return copy_to(piece(shard, i), piece(shard, i), wsr.at[n], wrl.at[n], (me, right))

    def to_left(shard, i, n):
        return copy_to(piece(shard, i), piece(shard, i), wsl.at[n], wrr.at[n], (me, left))

    def to_partner(ref, n):
        return copy_to(ref, ref, wps.at[n], wpr.at[n], (me, partner))

    local[4].wait()
    for n in range(3):
        strip_out(n).start()
    for n in range(4):
        to_right(dp, n, n).start()
        to_left(dp, (n + 2) % 4, n).start()
    to_partner(wbuf.at[dp], 0).start()
    for c in local[5:14]:
        c.wait()
    for c in local[14:]:
        c.start()

    def gate_step(p, carry):
        cols = pl.ds(pl.multiple_of(p * 256, 256), 256)
        sg[:, cols] = 1.0 / (1.0 + jnp.exp(-ogl_ref[:, cols].astype(F32)))
        return carry

    lax.fori_loop(0, PAIRS, gate_step, 0)

    pass_strip(0)
    table_in = jnp.concatenate(
        [ids_ref[...].astype(F32), group_ref[...], within_ref[...], jnp.zeros((C - 8, C), F32)], axis=0).T
    wide = lax.broadcasted_iota(jnp.int32, (C, DEVICES * CAP), 1)
    hits, targets, routes = [], [], []
    for n in range(2):
        expert = table_in[:, n:n + 1].astype(jnp.int32)
        dz = jnp.bitwise_and(jnp.right_shift(expert, 5) - z + 4, 3)
        dy = jnp.bitwise_and(jnp.right_shift(expert, 3) - y + 8, 3)
        dx = jnp.bitwise_and(jnp.right_shift(expert, 1) - x + 4, 3)
        dc = jnp.bitwise_and(expert - core + 2, 1)
        place = jnp.bitwise_and(dz + dy + dx, 3) * PER + dy * 8 + dx * 2 + dc
        group = jnp.right_shift(expert, 5)
        share = jnp.zeros((C, 1), F32)
        for i in range(4):
            share = share + jnp.where(group == i, table_in[:, 2 + i:3 + i], 0.0)
        routes.append(share * table_in[:, 6 + n:7 + n])
        targets.append(place * CAP)
        hits.append((lane == place).astype(F32))
    before = jnp.dot((lane < row_id).astype(BF16), (hits[0] + hits[1]).astype(BF16), preferred_element_type=F32)
    sent = jnp.zeros((C, DEVICES * CAP), F32)
    back = jnp.zeros((C, DEVICES * CAP), F32)
    for n in range(2):
        nth = jnp.sum(before * hits[n], axis=1, keepdims=True).astype(jnp.int32)
        chosen = wide == targets[n] + nth
        sent = sent + jnp.where(chosen, 1.0, 0.0)
        back = back + jnp.where(chosen, routes[n], 0.0)
    tab_send[...] = sent.astype(BF16)
    back_hi = back.astype(BF16)
    tab_back[0:C] = back_hi
    tab_back[C:2 * C] = (back - back_hi.astype(F32)).astype(BF16)

    fifteen(msg, rx1, sa, ra).wait_recv()

    spread = rx1[:, 0, :]
    in_f = gates[pl.ds(0, H, stride=4), :]
    in_b = gates[pl.ds(2, H, stride=4), :]
    fade_f = log_sigmoid(gates[pl.ds(1, H, stride=4), :] + rx1[:, 2, :]) + spread
    fade_b = log_sigmoid(gates[pl.ds(3, H, stride=4), :] + rx1[:, 3, :]) + spread
    upto = (row_id <= lane).astype(F32)
    since = (row_id >= lane).astype(F32)
    cum_f = jnp.dot(fade_f, upto, precision=HIGH, preferred_element_type=F32)
    cum_b = jnp.dot(fade_b, since, precision=HIGH, preferred_element_type=F32)
    end_f = jnp.broadcast_to(cum_f[:, C - 1:C], (H, C))
    end_b = jnp.broadcast_to(cum_b[:, 0:1], (H, C))
    w_f = jnp.exp(end_f - cum_f + in_f)
    w_b = jnp.exp(end_b - cum_b + in_b)
    rows[0] = cum_f - in_f
    rows[1] = cum_b - in_b
    rows[2] = jnp.exp(in_b)
    turned = jnp.concatenate([cum_f, cum_b, w_f, w_b, jnp.zeros((C - 4 * H, C), F32)], axis=0).T
    wf_hi = w_f.astype(BF16)
    wb_hi = w_b.astype(BF16)
    wf_lo = (w_f - wf_hi.astype(F32)).astype(BF16)
    wb_lo = (w_b - wb_hi.astype(F32)).astype(BF16)
    stacked = jnp.concatenate([wf_hi, wf_lo, wb_hi, wb_lo], axis=0)
    norm = jnp.dot(stacked, k_ref[...], preferred_element_type=F32)
    norm_f = norm[0:16] + norm[16:32]
    norm_b = norm[32:48] + norm[48:64]
    for p in range(PAIRS):
        h0, h1 = 2 * p, 2 * p + 1
        wpair[p, 0] = jnp.where(low_half, turned[:, 32 + h0:33 + h0], turned[:, 32 + h1:33 + h1])
        wpair[p, 1] = jnp.where(low_half, turned[:, 48 + h0:49 + h0], turned[:, 48 + h1:49 + h1])
        for h, keep in ((h0, low_row), (h1, ~low_row)):
            nf = norm_f[h:h + 1, p * C:(p + 1) * C]
            nb = norm_b[h:h + 1, p * C:(p + 1) * C]
            nf = jnp.where(keep, nf, pltpu.roll(nf, DK, 1))
            nb = jnp.where(keep, nb, pltpu.roll(nb, DK, 1))
            lsm[h] = jnp.concatenate(
                [nf, nb, end_f[h:h + 1], end_b[h:h + 1], jnp.zeros((4, C), F32)], axis=0)

    each_peer(lambda p: remote(lsm.at[p], rxm.at[me], sc.at[0], rc.at[0], p).start())
    rxm[me] = lsm[me]
    first = lax.div(me, 2) + 1

    def state_out(way, h, ssem, rsem):
        return remote(lst.at[h, way], rxs.at[me, way], ssem.at[0], rsem.at[0], h)

    def states_in(way, ssem, rsem):
        most = pl.ds(0, H - 1)
        return remote(lst.at[most, way], rxs.at[most, way], ssem.at[0], rsem.at[0], peer_of(1))

    def post_pair(i):
        p = lax.rem(first + i, PAIRS)
        for hh in range(2):
            h = 2 * p + hh

            @pl.when(h != me)
            def _():
                state_out(0, h, sb, rb).start()

    def state_step(i, carry):
        p = lax.rem(first + i, PAIRS)
        k32 = k_ref[:, pl.ds(pl.multiple_of(p * C, C), C)].astype(F32)
        both = jnp.concatenate([k32 * wpair[p, 0], k32 * wpair[p, 1]], axis=1).astype(BF16)
        vp = v_ref[:, pl.ds(pl.multiple_of(p * 256, 256), 256)]
        state = lax.dot_general(both, vp, TN, preferred_element_type=F32).astype(BF16)
        lst[2 * p, 0] = state[0:64, 0:128]
        lst[2 * p + 1, 0] = state[64:128, 128:256]
        lst[2 * p, 1] = state[128:192, 0:128]
        lst[2 * p + 1, 1] = state[192:256, 128:256]

        @pl.when(i > 0)
        def _():
            post_pair(i - 1)

        return carry

    lax.fori_loop(0, PAIRS, state_step, 0)
    post_pair(PAIRS - 1)
    each_peer(lambda p: state_out(1, p, sbb, rbb).start())
    rxs[me] = lst[me]

    def relay(n):
        to_right(left, n, n).wait_recv()
        to_right(left, n, 4 + n).start()
        to_left(right, n + 2, n).wait_recv()
        to_left(right, n + 2, 4 + n).start()


    for h in range(H):
        fcol[h] = jnp.broadcast_to(turned[:, h:h + 1], (C, C))
        bcol[h] = jnp.broadcast_to(turned[:, 16 + h:17 + h], (C, C))

    relay(0)

    def lhs_of(cols):
        qp = q_ref[:, cols] * jnp.asarray(DK ** -0.5, BF16)
        none = jnp.zeros_like(qp)
        return jnp.concatenate([jnp.where(low_half, qp, none), jnp.where(low_half, none, qp)], axis=0)

    def inner_step(p, carry):
        cols = pl.ds(pl.multiple_of(p * C, C), C)
        score2 = lax.dot_general(lhs_of(cols), k_ref[:, cols], NT, preferred_element_type=F32)
        for hh in range(2):
            h = 2 * p + hh
            score = score2[hh * C:(hh + 1) * C]
            ahead = fcol[h] - rows[0, pl.ds(h, 1), :]
            behind = bcol[h] - rows[1, pl.ds(h, 1), :]
            weighted = score * jnp.exp(jnp.where(earlier, ahead, behind))
            pf = jnp.where(earlier, weighted, 0.0)
            pb = jnp.where(earlier, jnp.where(diagonal, score * rows[2, pl.ds(h, 1), :], 0.0), weighted)
            both = jnp.concatenate([pf, pb], axis=0)
            zfb[h] = jnp.broadcast_to(jnp.sum(both, axis=1, keepdims=True), (2 * C, C))
            vcols = pl.ds(pl.multiple_of(h * DV, DV), DV)
            nfb[h] = jnp.dot(both.astype(BF16), v_ref[:, vcols], preferred_element_type=F32)
        return carry

    lax.fori_loop(0, PAIRS, inner_step, 0)

    relay(1)
    fifteen(lsm, rxm, sc, rc).wait_recv()
    enm[...] = jnp.zeros_like(enm)

    def slot(way, h):
        return est.at[lax.div(h, 2), way, pl.ds(pl.multiple_of(lax.rem(h, 2) * DK, DK), DK), :]

    def entry_out(way, p, ssem, rsem):
        return remote(ent.at[p, way], slot(way, me), ssem.at[0], rsem.at[me], p)

    def entry_in(way, p, ssem, rsem):
        return remote(ent.at[p, way], slot(way, p), ssem.at[0], rsem.at[p], p)

    def run(way, ssem, rsem, ssem_out, rsem_out):
        states_in(way, ssem, rsem).wait_recv()

        def carry_step(i, state):
            m, n = state
            c = i if way == 0 else H - 1 - i
            ent[c, way] = m.astype(BF16)
            enm[c, way:way + 1] = n
            keep = jnp.exp(rxm[c, 2 + way:3 + way])
            return m * keep + rxs[c, way].astype(F32), n * keep + rxm[c, way:way + 1]

        lax.fori_loop(0, H, carry_step, (jnp.zeros((DK, DV), F32), jnp.zeros((1, C), F32)))
        each_peer(lambda p: entry_out(way, p, ssem_out, rsem_out).start())

    run(0, sb, rb, se, re)
    run(1, sbb, rbb, seb, reb)
    each_peer(lambda p: remote(enm.at[p], esm.at[me], sd.at[0], rd.at[me], p).start())
    esm[me] = enm[me]
    est[lax.div(me, 2), :, pl.ds(pl.multiple_of(lax.rem(me, 2) * DK, DK), DK), :] = ent[me]
    pass_strip(1)
    pass_strip(2)


    def outer_step(i, carry):
        p = lax.rem(lax.div(me, 2) + PAIRS - i, PAIRS)
        for hh in range(2):
            h = 2 * p + hh

            @pl.when(h != me)
            def _():
                remote(enm.at[h], esm.at[h], sd.at[0], rd.at[h], h).wait_recv()
                entry_in(0, h, se, re).wait_recv()
                entry_in(1, h, seb, reb).wait_recv()

        cols = pl.ds(pl.multiple_of(p * C, C), C)
        lhs = lhs_of(cols)
        carried = jnp.dot(lhs, jnp.concatenate([est[p, 0], est[p, 1]], axis=1), preferred_element_type=F32)
        nf_row = jnp.where(low_row, esm[2 * p, 0:1], esm[2 * p + 1, 0:1])
        nb_row = jnp.where(low_row, esm[2 * p, 1:2], esm[2 * p + 1, 1:2])
        lhs32 = lhs.astype(F32)
        zf_all = jnp.sum(lhs32 * nf_row, axis=1, keepdims=True)
        zb_all = jnp.sum(lhs32 * nb_row, axis=1, keepdims=True)
        for hh in range(2):
            h = 2 * p + hh
            part = slice(hh * C, (hh + 1) * C)
            grow_f = jnp.exp(fcol[h])
            grow_b = jnp.exp(bcol[h])
            zf = zfb[h, 0:C] + grow_f * zf_all[part]
            zb = zfb[h, C:2 * C] + grow_b * zb_all[part]
            nf = nfb[h, 0:C] + grow_f * carried[part, 0:DV]
            nb = nfb[h, C:2 * C] + grow_b * carried[part, DV:2 * DV]
            total = nf / jnp.maximum(jnp.abs(zf), 1.0) + nb / jnp.maximum(jnp.abs(zb), 1.0)
            mean = jnp.mean(total * total, axis=1, keepdims=True)
            mixed = (total * lax.rsqrt(mean + EPS) * rx1[h, 1:2]).astype(BF16)
            vcols = pl.ds(pl.multiple_of(h * DV, DV), DV)
            gated[:, vcols] = (mixed.astype(F32) * sg[:, vcols]).astype(BF16)
        return carry

    lax.fori_loop(0, PAIRS, outer_step, 0)

    def project(shard):
        cols = pl.ds(pl.multiple_of(shard * 256, 256), 256)
        proj[:, cols] = jnp.dot(gated[...], wbuf[shard], preferred_element_type=F32)

    for n in range(1, 8):
        pl.semaphore_signal(meet, inc=1, device_id=(me, lax.rem(dp + n, 8)), device_id_type=MESH)
    each_peer(lambda p: pl.semaphore_signal(meet, inc=1, device_id=(p, dp), device_id_type=MESH))
    project(dp)
    for n in range(2, 4):
        to_right(left, n, n).wait_recv()
        to_left(right, n - 2, n).wait_recv()
    strips(0).wait_recv()
    to_partner(wbuf.at[left], 1).start()
    project(left)
    strips(1).wait_recv()
    to_partner(wbuf.at[right], 2).start()
    project(right)
    strips(2).wait_recv()
    edge = pl.ds(0, BASE)
    to_partner(wbuf.at[across, edge, :], 3).start()
    far = 1 - 2 * core
    to_partner(wbuf.at[partner], 0).wait_recv()
    project(partner)
    for n in range(2):
        to_right(across, n, 4 + n).wait_recv()
        to_partner(piece(across, n), 4 + n).start()
        to_left(across, n + 2, 4 + n).wait_recv()
        to_partner(piece(across, n + 2), 6 + n).start()
    to_partner(wbuf.at[left + far], 1).wait_recv()
    project(left + far)
    to_partner(wbuf.at[right + far], 2).wait_recv()
    project(right + far)
    project(across)
    to_partner(wbuf.at[across + far, edge, :], 3).wait_recv()
    for n in range(2):
        to_partner(piece(across + far, n), 4 + n).wait_recv()
        to_partner(piece(across + far, n + 2), 6 + n).wait_recv()
    project(across + far)

    local[14].wait()
    pr = proj[...]
    scale = lax.rsqrt(jnp.mean(pr * pr, axis=1, keepdims=True) + EPS)
    stream = (res_ref[...].astype(F32) + cng_ref[...] * pr * scale).astype(BF16).astype(F32)
    proj[...] = stream
    scale = lax.rsqrt(jnp.mean(stream * stream, axis=1, keepdims=True) + EPS)
    gated[...] = (eng_ref[...] * stream * scale).astype(BF16)

    def route_of(j, i):
        t = lax.rem(i * STRIDE, PER)
        dc = lax.rem(t, 2)
        dx = lax.rem(lax.div(t, 2), 4)
        dy = lax.div(t, 8)
        dz = lax.rem(j + 8 - dx - dy, 4)
        return j * PER + t, dz, dy, dx, dc

    def onward(j, i):
        place, dz, dy, dx, dc = route_of(j, i)
        sp_to = lax.rem(z + dz, 4) * 4 + lax.rem(y + dy, 4)
        dp_to = lax.rem(x + dx, 4) * 2 + lax.rem(core + dc, 2)
        return place, (sp_to, dp_to)

    def homeward(j, i):
        place, dz, dy, dx, dc = route_of(j, i)
        sp_to = lax.rem(z + 4 - dz, 4) * 4 + lax.rem(y + 4 - dy, 4)
        dp_to = lax.rem(x + 4 - dx, 4) * 2 + lax.rem(core + dc, 2)
        return place, (sp_to, dp_to)

    def send_chunk(j, way, src, dst, ssem, rsem):
        def step(i, carry):
            place, where = way(j, i)

            @pl.when(place != 0)
            def _():
                copy_to(src.at[place], dst.at[place], ssem.at[j], rsem.at[j], where).start()

            return carry

        lax.fori_loop(0, PER, step, 0)

    def whole(j, src, dst, ssem, rsem):
        span = pl.ds(1, PER - 1) if j == 0 else pl.ds(j * PER, PER)
        return copy_to(src.at[span], dst.at[span], ssem.at[j], rsem.at[j], (me, partner))

    for j in range(CHUNKS):
        rows_out = lax.dot_general(
            tab_send[:, j * C:(j + 1) * C], gated[...], TN, preferred_element_type=F32)
        outgoing[j * PER:(j + 1) * PER] = rows_out.astype(BF16).reshape(PER, CAP, D)
        if j == 0:
            pl.semaphore_wait(meet, H - 1 + 7)
        send_chunk(j, onward, outgoing, arrived, ds, dr)
        if j == 0:
            arrived[0] = outgoing[0]

    for c in local[15:]:
        c.wait()
    fifteen(msg, rx1, sa, ra).wait_send()
    fifteen(lsm, rxm, sc, rc).wait_send()
    states_in(0, sb, rb).wait_send()
    states_in(1, sbb, rbb).wait_send()
    fifteen(enm, esm, sd, rc).wait_send()
    states_in(0, se, rb).wait_send()
    states_in(1, seb, rbb).wait_send()
    for n in range(6):
        to_right(dp, 0, n).wait_send()
        to_left(dp, 0, n).wait_send()
    for n in range(3):
        to_partner(wbuf.at[dp], n).wait_send()
    to_partner(wbuf.at[dp, edge, :], 3).wait_send()
    for n in range(4, 8):
        to_partner(piece(dp, 0), n).wait_send()
    for n in range(3):
        strip_out(n).wait_send()
        strips(n).wait_send()

    def expert_chunk(j):
        rows_in = arrived[pl.ds(j * PER, PER)].reshape(PER * CAP, D)
        a = jnp.dot(rows_in, gate_w[...], preferred_element_type=F32)
        b = jnp.dot(rows_in, up_w[...], preferred_element_type=F32)
        hidden = (a / (1.0 + jnp.exp(-a)) * b).astype(BF16)
        made = jnp.dot(hidden, down_w[...], preferred_element_type=F32).astype(BF16)
        produced[pl.ds(j * PER, PER)] = made.reshape(PER, CAP, D)

    def expert_step(j, carry):
        for n in range(CHUNKS):
            @pl.when(j == n)
            def _():
                whole(n, outgoing, arrived, ds, dr).wait_recv()

        @pl.when(j >= 1)
        def _():
            send_chunk(j - 1, homeward, produced, returned, bs, br)

        expert_chunk(j)
        return carry

    lax.fori_loop(0, CHUNKS, expert_step, 0)
    for j in range(CHUNKS - 1, CHUNKS):
        send_chunk(j, homeward, produced, returned, bs, br)
    returned[0] = produced[0]
    for j in range(CHUNKS):
        whole(j, outgoing, arrived, ds, dr).wait_send()

    for j in range(CHUNKS):
        whole(j, produced, returned, bs, br).wait_recv()
        rows_back = returned[j * PER:(j + 1) * PER].reshape(PER * CAP, D)
        parts = jnp.dot(tab_back[:, j * C:(j + 1) * C], rows_back, preferred_element_type=F32)
        proj[...] += parts[0:C] + parts[C:2 * C]
    out_ref[...] = proj[...].astype(BF16)

    for j in range(CHUNKS):
        whole(j, produced, returned, bs, br).wait_send()


def on_device(
    residual_input, queries, keys, values, gate_logits, retention_offset, log_forget_extra,
    lane_amplifier, output_gate_logits, output_projection, cell_norm_gain, expert_norm_gain,
    expert_index, group_mixing_weight, within_group_weight, gate_weight, up_weight, down_weight,
):
    vm = pl.BlockSpec(memory_space=pltpu.VMEM)
    hbm = pl.BlockSpec(memory_space=pl.ANY)
    dma = pltpu.SemaphoreType.DMA
    small = pltpu.VMEM((H, 8, C), F32)
    state = pltpu.VMEM((H, 2, DK, DV), BF16)
    slots = pltpu.VMEM((DEVICES, CAP, D), BF16)
    out = pl.pallas_call(
        layer_kernel,
        out_shape=jax.ShapeDtypeStruct((C, D), BF16),
        in_specs=[hbm] * 18,
        out_specs=vm,
        scratch_shapes=[
            pltpu.VMEM((4 * H, C), BF16),
            pltpu.VMEM((H, C), F32),
            pltpu.VMEM((1, C), F32),
            pltpu.VMEM((1, 2), F32),
            pltpu.VMEM((2, C), jnp.int32),
            pltpu.VMEM((4, C), F32),
            pltpu.VMEM((2, C), F32),
            pltpu.VMEM((1, D), F32),
            pltpu.VMEM((1, D), F32),
            pltpu.VMEM((C, H * DK), BF16),
            pltpu.VMEM((C, H * DK), BF16),
            pltpu.VMEM((C, H * DV), BF16),
            pltpu.VMEM((C, H * DV), BF16),
            pltpu.VMEM((C, D), BF16),
            pltpu.VMEM((8, D, 256), BF16),
            pltpu.VMEM((D, FF), BF16),
            pltpu.VMEM((D, FF), BF16),
            pltpu.VMEM((FF, D), BF16),
            small, small, state, small, state, small, state, small,
            pltpu.VMEM((PAIRS, 2, 2 * DK, DV), BF16),
            small,
            pltpu.VMEM((4 * H, C), F32),
            pltpu.VMEM((H, C, C), F32),
            pltpu.VMEM((H, C, C), F32),
            pltpu.VMEM((3, H, C), F32),
            pltpu.VMEM((PAIRS, 2, C, C), F32),
            pltpu.VMEM((H, 2 * C, DV), F32),
            pltpu.VMEM((H, 2 * C, C), F32),
            pltpu.VMEM((C, H * DV), F32),
            pltpu.VMEM((C, H * DV), BF16),
            pltpu.VMEM((C, D), F32),
            pltpu.VMEM((C, DEVICES * CAP), BF16),
            pltpu.VMEM((2 * C, DEVICES * CAP), BF16),
            slots, slots, slots, slots,
            dma((18,)),
        ] + [dma((1,))] * 9 + [dma((H,)), dma((1,)), dma((H,)), dma((1,)), dma((H,))] + [dma((6,))] * 4 + [dma((8,))] * 2 + [dma((3,))] * 4 + [dma((CHUNKS,))] * 4 + [pltpu.SemaphoreType.REGULAR],
        compiler_params=pltpu.CompilerParams(
            collective_id=0, has_side_effects=True, vmem_limit_bytes=67_043_328),
        name="layer",
    )(
        queries[0], keys[0], values[0], output_gate_logits[0], residual_input[0], output_projection,
        gate_weight[0], up_weight[0], down_weight[0],
        gate_logits[0].T, log_forget_extra.reshape(H, C), lane_amplifier.reshape(1, C), retention_offset,
        expert_index[0].T, group_mixing_weight[0].T, within_group_weight[0].T,
        cell_norm_gain.reshape(1, D), expert_norm_gain.reshape(1, D),
    )
    return out.reshape(1, C, D)


def solution(mesh):
    by_place = P("dp", "sp", None)
    by_expert = P(("sp", "dp"), None, None)
    in_specs = (
        by_place, by_place, by_place, by_place, by_place, P("sp", None), by_place, P("sp"), by_place,
        P(None, "dp"), P(), P(), by_place, by_place, by_place, by_expert, by_expert, by_expert,
    )
    return jax.shard_map(on_device, mesh=mesh, in_specs=in_specs, out_specs=by_place, check_vma=False)
```
